32 devices in a mesh: sp: 16 (over z, y, x), tp: 2 (over core).
Axes of the slice: x: 2, y: 2, z: 4, core: 2. Of those that a mesh axis runs over, the one named last changes fastest.
Arguments:
- prompt: bfloat16 [1, 8192, 2048], P(None, 'sp', 'tp'), may hold values from -6 to 6
- new_token: bfloat16 [1, 2048], P(None, 'tp'), may hold values from -6 to 6
- w_query: bfloat16 [2048, 2048], P(None, 'tp'), may hold values from -0.125 to 0.125
- w_key: bfloat16 [2048, 2048], P(None, 'tp'), may hold values from -0.125 to 0.125
- w_value: bfloat16 [2048, 2048], P(None, 'tp'), may hold values from -0.125 to 0.125
- decay_rate: float32 [16], P('tp'), may hold values from 1e-05 to 0.06
- norm_gain: float32 [2048], P('tp'), may hold values from 0.1 to 1.9
Outputs:
- mixed: bfloat16 [1, 8192, 2048], P(None, 'sp', 'tp')
- cache: bfloat16 [1, 16, 128, 128], P(None, 'tp', 'sp')
- new_read: bfloat16 [1, 2048], P(None, 'tp')
The draws below stay inside these ranges and needn't reach their ends.
All inputs are finite; a program needn't handle non-finite values.
Results may differ from the reference program's by a relative error of at most 0.0083.
Values may be sent and summed in bfloat16 or wider, within the bound.
No kernel may reach another device: no remote copies, remote signals or barrier semaphores. Data moves between devices by JAX's collectives and lax.ppermute only.
A program may use at most 64 MiB of HBM per device.

```python
import jax
import jax.numpy as jnp
from jax import lax

D = 2048
H = 16
HEAD = 128
SEQS = 1
POS_DEV = 512
LEN = 8192


def draw_decay_rate(key, part):
    lowest = 1e-05
    highest = 0.06
    uniform_draw = jax.random.uniform(key, (H,), jnp.float32)
    return jnp.exp(jnp.log(lowest) + uniform_draw * (jnp.log(highest) - jnp.log(lowest)))


def shard_levels(rng, extent, pieces, smallest, high):
    def one(position, blocks):
        heights = jax.random.uniform(jax.random.fold_in(jax.random.fold_in(rng, 6), position), (blocks,), jnp.float32, smallest / len(pieces), high / len(pieces))
        return jnp.repeat(jnp.exp(heights), extent[position] // blocks).reshape((-1,) + (1,) * (len(extent) - position - 1))

    level = one(*pieces[0])
    for cut in pieces[1:]:
        level = level * one(*cut)
    return level


def gaussian(rng, shape, scale, reach, shards=(), held_as=jnp.bfloat16):
    result = jax.random.normal(rng, shape, jnp.float32) * scale
    if len(shards) > 0:
        result = shard_levels(rng, shape, shards, -0.22, 0.18) * result
    return jnp.clip(result, min=-reach, max=reach).astype(held_as)


def setup_inputs(seed: int = 0) -> dict:
    seeds = jax.random.split(jax.random.key(seed), 8)
    return {
        "prompt": gaussian(seeds[0], (SEQS, LEN, D), 1.0, 6.0, ((1, 16), (2, 2))),
        "new_token": gaussian(seeds[1], (SEQS, D), 1.0, 6.0, ((1, 2),)),
        "w_query": gaussian(seeds[2], (D, H * HEAD), D ** -0.5, 0.125, ((1, 2),)),
        "w_key": gaussian(seeds[3], (D, H * HEAD), D ** -0.5, 0.125, ((1, 2),)),
        "w_value": gaussian(seeds[4], (D, H * HEAD), D ** -0.5, 0.125, ((1, 2),)),
        "decay_rate": draw_decay_rate(jax.random.fold_in(seeds[7], 71), 0),
        "norm_gain": jnp.clip(1.0 + 0.18 * jax.random.normal(seeds[6], (H * HEAD,), jnp.float32), 0.1, 1.9),
    }


rope_base = 10000.0
norm_floor = 1e-05

def rotate(tensor, positions):
    head_width = tensor.shape[-1]
    inverse = rope_base ** (-jnp.arange(0, head_width, 2, dtype=jnp.float32) / head_width)
    angles = positions.astype(jnp.float32)[:, None] * inverse[None, :]
    cosine = jnp.cos(angles)[:, None, :]
    sine_part = jnp.sin(angles)[:, None, :]
    first_half = tensor[..., :head_width // 2]
    second_half = tensor[..., head_width // 2:]
    return jnp.concatenate([first_half * cosine - second_half * sine_part, first_half * sine_part + second_half * cosine], axis=-1)

def head_norm(output, gain):
    center = lax.optimization_barrier(jnp.mean(output, axis=-1, keepdims=True))
    spread = lax.optimization_barrier(jnp.mean(jnp.square(output - center), axis=-1, keepdims=True))
    return (output - center) * lax.rsqrt(spread + norm_floor) * gain

def decay_tables(log_gamma, block_size):
    offsets = jnp.arange(block_size, dtype=jnp.float32)
    gap_table = offsets[:, None] - offsets[None, :]
    within = jnp.where(gap_table[None] >= 0, jnp.exp(jnp.maximum(gap_table, 0.0)[None] * log_gamma[:, None, None]), 0.0)
    query_decay = jnp.exp((offsets[:, None] + 1.0) * log_gamma[None, :])
    key_decay = jnp.exp((block_size - 1.0 - offsets[:, None]) * log_gamma[None, :])
    return (within, query_decay, key_decay)

def project(token_rows, weight):
    return jnp.dot(token_rows, weight, preferred_element_type=jnp.float32).astype(jnp.bfloat16)

def reference(prompt, new_token, w_query, w_key, w_value, decay_rate, norm_gain):
    sequences, length, model_width = prompt.shape
    block_size = POS_DEV
    blocks = length // block_size
    token_rows = prompt.reshape(sequences * length, model_width)
    full_shape = (sequences, length, H, HEAD)
    queries = project(token_rows, w_query).reshape(full_shape)
    key_rows = project(token_rows, w_key).reshape(full_shape)
    values = project(token_rows, w_value).reshape(full_shape)
    positions = jnp.arange(length, dtype=jnp.int32)
    scaled = (rotate(queries.astype(jnp.float32), positions) * HEAD ** (-0.5)).astype(jnp.bfloat16)
    turned = rotate(key_rows.astype(jnp.float32), positions).astype(jnp.bfloat16)
    log_gamma = -decay_rate
    within, query_decay, key_decay = decay_tables(log_gamma, block_size)
    block_shape = (sequences, blocks, block_size, H, HEAD)

    def to_blocks(tensor):
        return jnp.moveaxis(tensor.reshape(block_shape), 1, 0)
    weighted = (to_blocks(turned).astype(jnp.float32) * key_decay[None, None, :, :, None]).astype(jnp.bfloat16)
    factor = jnp.exp(block_size * log_gamma)

    def advance(state_now, inputs):
        query_block, key_block, weighted_block, value_block = inputs
        scores = jnp.einsum('snhd,smhd->shnm', query_block.astype(jnp.float32), key_block.astype(jnp.float32)) * within[None]
        scores = lax.optimization_barrier(scores.astype(jnp.bfloat16)).astype(jnp.float32)
        inner_part = jnp.einsum('shnm,smhe->snhe', scores, value_block.astype(jnp.float32))
        state_read = lax.optimization_barrier(state_now.astype(jnp.bfloat16)).astype(jnp.float32)
        carried = jnp.einsum('snhd,shde->snhe', query_block.astype(jnp.float32), state_read) * query_decay[None, :, :, None]
        local_state = jnp.einsum('smhd,smhe->shde', weighted_block.astype(jnp.float32), value_block.astype(jnp.float32))
        return (state_now * factor[None, :, None, None] + local_state, inner_part + carried)
    initial = jnp.zeros((sequences, H, HEAD, HEAD), jnp.float32)
    final_state, outputs = lax.scan(advance, initial, (to_blocks(scaled), to_blocks(turned), weighted, to_blocks(values)))
    outputs = jnp.moveaxis(outputs, 0, 1).reshape(full_shape)
    gain = norm_gain.reshape(H, HEAD)
    mixed = head_norm(outputs, gain).astype(jnp.bfloat16).reshape(sequences, length, H * HEAD)
    cache = final_state.astype(jnp.bfloat16)
    token_shape = (sequences, 1, H, HEAD)
    token_query = project(new_token, w_query).reshape(token_shape)
    token_key = project(new_token, w_key).reshape(token_shape)
    token_value = project(new_token, w_value).reshape(token_shape)
    token_positions = jnp.full((1,), length, jnp.int32)
    token_scaled = (rotate(token_query.astype(jnp.float32), token_positions) * HEAD ** (-0.5)).astype(jnp.bfloat16)[:, 0]
    token_turned = rotate(token_key.astype(jnp.float32), token_positions).astype(jnp.bfloat16)[:, 0]
    from_cache = jnp.einsum('shd,shde->she', token_scaled.astype(jnp.float32), final_state, precision=lax.Precision.HIGHEST)
    own_score = lax.optimization_barrier(jnp.sum(token_scaled.astype(jnp.float32) * token_turned.astype(jnp.float32), axis=-1, keepdims=True))
    read_out = jnp.exp(log_gamma)[None, :, None] * from_cache + own_score * token_value[:, 0].astype(jnp.float32)
    new_read = head_norm(read_out, gain).astype(jnp.bfloat16).reshape(sequences, H * HEAD)
    return (mixed, cache, new_read)
```

```python
import jax
import jax.numpy as jnp
from jax import lax
from jax.experimental import pallas as pl
from jax.experimental.pallas import tpu as pltpu
from jax.sharding import PartitionSpec as P

HEAD = 128


rope_base = 10000.0
norm_floor = 1e-05


def rotate(tensor, positions):
    head_width = tensor.shape[-1]
    inverse = rope_base ** (-jnp.arange(0, head_width, 2, dtype=jnp.float32) / head_width)
    angles = positions.astype(jnp.float32)[:, None] * inverse[None, :]
    cosine = jnp.cos(angles)[:, None, :]
    sine_part = jnp.sin(angles)[:, None, :]
    first_half = tensor[..., : head_width // 2]
    second_half = tensor[..., head_width // 2 :]
    return jnp.concatenate(
        [
            first_half * cosine - second_half * sine_part,
            first_half * sine_part + second_half * cosine,
        ],
        axis=-1,
    )


def head_norm(output, gain):
    center = jnp.mean(output, axis=-1, keepdims=True)
    spread = jnp.mean(jnp.square(output - center), axis=-1, keepdims=True)
    return (output - center) * lax.rsqrt(spread + norm_floor) * gain


def decay_tables(log_gamma, block_size):
    offsets = jnp.arange(block_size, dtype=jnp.float32)
    gap_table = offsets[:, None] - offsets[None, :]
    within = jnp.where(
        gap_table[None] >= 0,
        jnp.exp(jnp.maximum(gap_table, 0.0)[None] * log_gamma[:, None, None]),
        0.0,
    )
    query_decay = jnp.exp((offsets[:, None] + 1.0) * log_gamma[None, :])
    key_decay = jnp.exp((block_size - 1.0 - offsets[:, None]) * log_gamma[None, :])
    return (within, query_decay, key_decay)


def plain_device(prompt, new_token, w_query, w_key, w_value, decay_rate, norm_gain):
    sequences, block_size, feature_part = prompt.shape
    head_count = w_query.shape[1] // HEAD
    members = lax.axis_size("sp")
    device_rank = lax.axis_index("sp")
    prompt_rows = sequences * block_size
    token_rows = jnp.concatenate([prompt.reshape(prompt_rows, feature_part), new_token], axis=0)
    weight_list = (w_query, w_key, w_value)
    shard_piece = lax.all_gather(token_rows, "tp", axis=1, tiled=True)
    projected = tuple(
        (jnp.dot(shard_piece, weight, preferred_element_type=jnp.float32) for weight in weight_list)
    )
    full_shape = (sequences, block_size, head_count, HEAD)
    queries, key_rows, values = [
        tensor[:prompt_rows].astype(jnp.bfloat16).reshape(full_shape) for tensor in projected
    ]
    token_query, token_key, token_value = [
        tensor[prompt_rows:].astype(jnp.bfloat16).reshape(sequences, 1, head_count, HEAD)
        for tensor in projected
    ]
    positions = device_rank * block_size + jnp.arange(block_size, dtype=jnp.int32)
    scaled = (rotate(queries.astype(jnp.float32), positions) * HEAD ** (-0.5)).astype(jnp.bfloat16)
    turned = rotate(key_rows.astype(jnp.float32), positions).astype(jnp.bfloat16)
    log_gamma = -decay_rate
    within, query_decay, key_decay = decay_tables(log_gamma, block_size)
    weighted = (turned.astype(jnp.float32) * key_decay[None, :, :, None]).astype(jnp.bfloat16)
    local_state = jnp.einsum(
        "smhd,smhe->shde", weighted, values, preferred_element_type=jnp.float32
    )
    pieces = lax.all_to_all(local_state[None], "sp", split_axis=3, concat_axis=0, tiled=True)
    source_index = jnp.arange(members, dtype=jnp.float32)
    gap_table = source_index[:, None] - 1.0 - source_index[None, :]
    weights = jnp.where(
        gap_table[None] >= 0,
        jnp.exp(jnp.maximum(gap_table, 0.0)[None] * block_size * log_gamma[:, None, None]),
        0.0,
    )
    prefix = jnp.einsum("hji,ishre->jshre", weights, pieces, precision=lax.Precision.HIGHEST)
    tail_all = jnp.exp((members - 1.0 - source_index)[None, :] * block_size * log_gamma[:, None])
    final_rows = jnp.einsum("hi,ishre->shre", tail_all, pieces, precision=lax.Precision.HIGHEST)
    incoming = lax.all_to_all(
        prefix.astype(jnp.bfloat16), "sp", split_axis=0, concat_axis=3, tiled=True
    ).astype(prefix.dtype)[0]
    scores = (
        jnp.einsum("snhd,smhd->shnm", scaled, turned, preferred_element_type=jnp.float32)
        * within[None]
    )
    inner_part = jnp.einsum(
        "shnm,smhe->snhe", scores.astype(jnp.bfloat16), values, preferred_element_type=jnp.float32
    )
    carried = (
        jnp.einsum(
            "snhd,shde->snhe",
            scaled,
            incoming.astype(jnp.bfloat16),
            preferred_element_type=jnp.float32,
        )
        * query_decay[None, :, :, None]
    )
    gain = norm_gain.reshape(head_count, HEAD)
    mixed = (
        head_norm(inner_part + carried, gain)
        .astype(jnp.bfloat16)
        .reshape(sequences, block_size, head_count * HEAD)
    )
    cache = final_rows.astype(jnp.bfloat16)
    token_positions = jnp.full((1,), block_size * members, jnp.int32)
    token_scaled = (
        rotate(token_query.astype(jnp.float32), token_positions) * HEAD ** (-0.5)
    ).astype(jnp.bfloat16)[:, 0]
    token_turned = rotate(token_key.astype(jnp.float32), token_positions).astype(jnp.bfloat16)[:, 0]
    row_count = final_rows.shape[2]
    query_rows = lax.dynamic_slice_in_dim(
        token_scaled, device_rank * row_count, row_count, 2
    ).astype(jnp.float32)
    partial_value = jnp.einsum(
        "shr,shre->she", query_rows, final_rows, precision=lax.Precision.HIGHEST
    )
    read_sum = lax.psum(partial_value, "sp")
    own_score = jnp.sum(
        token_scaled.astype(jnp.float32) * token_turned.astype(jnp.float32), axis=-1, keepdims=True
    )
    read_out = jnp.exp(log_gamma)[None, :, None] * read_sum + own_score * token_value[:, 0].astype(
        jnp.float32
    )
    new_read = head_norm(read_out, gain).astype(jnp.bfloat16).reshape(sequences, head_count * HEAD)
    return (mixed, cache, new_read)


PLANE = 4
TOKEN_ROWS = 16
f32 = jnp.float32
bf16 = jnp.bfloat16


def vmem():
    return pl.BlockSpec(memory_space=pltpu.VMEM)


def smem():
    return pl.BlockSpec(memory_space=pltpu.SMEM)


def hbm():
    return pl.BlockSpec(memory_space=pltpu.HBM)


def params(**extra):
    return pltpu.CompilerParams(vmem_limit_bytes=24 * 1024 * 1024, **extra)


def shape(dims, dtype):
    return jax.ShapeDtypeStruct(dims, dtype)


def load_rows(place, own, other, token_own, token_other, rows, sems):
    count, part = own.shape

    for rank in range(2):

        @pl.when(place[0] == rank)
        def _():
            near = pl.ds(rank * part, part)
            far = pl.ds((1 - rank) * part, part)
            first = pltpu.make_async_copy(own, rows.at[pl.ds(0, count), near], sems.at[0])
            second = pltpu.make_async_copy(other, rows.at[pl.ds(0, count), far], sems.at[1])
            first.start()
            second.start()
            tail = (TOKEN_ROWS, part)
            rows[pl.ds(count, TOKEN_ROWS), near] = jnp.broadcast_to(token_own[...], tail)
            rows[pl.ds(count, TOKEN_ROWS), far] = jnp.broadcast_to(token_other[...], tail)
            first.wait()
            second.wait()


def turn(rows, cosine, sine):
    return rows * cosine + pltpu.roll(rows, HEAD // 2, axis=1) * sine


def into_parts(matrix, parts, outer):
    rest = HEAD // (outer * PLANE)
    split = matrix.reshape(outer, PLANE, rest, HEAD)
    for member in range(PLANE):
        parts[member] = split[:, member].reshape(outer * rest, HEAD)


def key_value_kernel(outer, place, rate, own, other, token_own, token_other, w_key, w_value, cosine, sine,
                     turned, values, token_key, token_value, *tail):
    pieces, (rows, parts, sems) = tail[:PLANE], tail[PLANE:]
    step = pl.program_id(0)
    count = own.shape[0]

    @pl.when(step == 0)
    def _():
        load_rows(place, own, other, token_own, token_other, rows, sems)

    key_rows = jnp.dot(rows[...], w_key[...], preferred_element_type=f32).astype(bf16).astype(f32)
    value_rows = jnp.dot(rows[...], w_value[...], preferred_element_type=f32).astype(bf16)
    values[...] = value_rows[:count]
    token_value[...] = value_rows[count:]
    offsets = lax.broadcasted_iota(jnp.int32, (count, HEAD), 0).astype(f32)
    for lane in range(w_key.shape[1] // HEAD):
        columns = slice(lane * HEAD, (lane + 1) * HEAD)
        result = turn(key_rows[:, columns], cosine[...], sine[...]).astype(bf16)
        turned[:, columns] = result[:count]
        token_key[:, columns] = result[count:]
        head_rate = rate[step * (w_key.shape[1] // HEAD) + lane]
        decay = jnp.exp((count - 1.0 - offsets) * -head_rate)
        weighted = (result[:count].astype(f32) * decay).astype(bf16)
        local = lax.dot_general(weighted, value_rows[:count, columns], (((0,), (0,)), ((), ())), preferred_element_type=f32)
        into_parts(local, parts, outer)
        for r in range(PLANE):
            pieces[r][lane] = parts[place[1 + r]].astype(bf16)


def query_kernel(outer, place, own, other, token_own, token_other, w_query, cosine, sine,
                 scaled, token_scaled, token_rows, rows, parts, sems):
    count = own.shape[0]

    @pl.when(pl.program_id(0) == 0)
    def _():
        load_rows(place, own, other, token_own, token_other, rows, sems)

    queries = jnp.dot(rows[...], w_query[...], preferred_element_type=f32).astype(bf16).astype(f32)
    for lane in range(w_query.shape[1] // HEAD):
        columns = slice(lane * HEAD, (lane + 1) * HEAD)
        result = (turn(queries[:, columns], cosine[...], sine[...]) * HEAD ** (-0.5)).astype(bf16)
        scaled[:, columns] = result[:count]
        token_scaled[:, columns] = result[count:]
        token = jnp.broadcast_to(result[count:].astype(f32)[:1], (HEAD, HEAD))
        into_parts(token.T, parts, outer)
        token_rows[lane] = parts[place[1]]


def inner_kernel(rate, scaled, turned, values, inner):
    step = pl.program_id(0)
    count, width = scaled.shape
    half = count // 2
    lanes = lax.broadcasted_iota(jnp.int32, (8, count), 1).astype(f32)
    keep = lax.broadcasted_iota(jnp.int32, (half, half), 0) >= lax.broadcasted_iota(jnp.int32, (half, half), 1)
    for lane in range(width // HEAD):
        columns = slice(lane * HEAD, (lane + 1) * HEAD)
        growth = jnp.exp(lanes * rate[step * (width // HEAD) + lane])[:1]

        def products(n, m):
            raw = lax.dot_general(scaled[n * half:(n + 1) * half, columns], turned[m * half:(m + 1) * half, columns],
                                  (((1,), (1,)), ((), ())), preferred_element_type=f32)
            raw = raw * growth[:, m * half:(m + 1) * half]
            return (jnp.where(keep, raw, 0.0) if n == m else raw).astype(bf16)

        low, high = values[:half, columns], values[half:, columns]
        inner[:half, columns] = jnp.dot(products(0, 0), low, preferred_element_type=f32)
        inner[half:, columns] = jnp.dot(products(1, 0), low, preferred_element_type=f32) + jnp.dot(
            products(1, 1), high, preferred_element_type=f32)


def plane_kernel(count, place, rate, *refs):
    pieces, (total, before, parts) = refs[:PLANE], refs[PLANE:]
    for r in range(PLANE):
        parts[place[1 + r]] = pieces[r][...].astype(f32)
    for head in range(total.shape[0]):
        factor = jnp.exp(jnp.full(total.shape[1:], -rate[head] * count, f32))
        state = jnp.zeros(total.shape[1:], f32)
        for member in range(PLANE):
            before[member, head] = state
            state = state * factor + parts[member, head]
        total[head] = state.astype(bf16)


def line_kernel(count, outer, place, line, rate, *refs):
    totals = refs[:outer]
    before, token_rows = refs[outer:outer + 2]
    results, cache = refs[outer + 2:outer + 2 + PLANE], refs[outer + 2 + PLANE]
    ordered, running, final, reads = refs[outer + 3 + PLANE:]
    heads, width = totals[0].shape[:2]
    for s in range(outer):
        ordered[line[s]] = totals[s][...].astype(f32)
    for head in range(heads):
        log_factor = jnp.full((width, HEAD), -rate[head] * count, f32)
        factor = jnp.exp(log_factor * PLANE)
        state = jnp.zeros((width, HEAD), f32)
        for member in range(outer):
            running[member] = state
            state = state * factor + ordered[member, head]
        final[...] = state.reshape(final.shape)
        cache[head] = final[line[0]].astype(bf16)
        read = jnp.sum(token_rows[head] * state, axis=0, keepdims=True)
        high = read.astype(bf16).astype(f32)
        reads[pl.ds(head, 1), :] = high
        reads[pl.ds(heads + head, 1), :] = read - high
        arriving = running[line[0]]
        for r in range(PLANE):
            scale = jnp.exp(log_factor * place[1 + r].astype(f32))
            results[r][pl.ds(head * width, width), :] = (before[place[1 + r], head] + scale * arriving).astype(bf16)
    for r in range(PLANE):
        results[r][pl.ds(heads * width, 2 * heads), :] = reads[...].astype(bf16)


def finish(rows, gain):
    center = jnp.mean(rows, axis=-1, keepdims=True)
    rows = rows - center
    spread = jnp.mean(jnp.square(rows), axis=-1, keepdims=True)
    return rows * lax.rsqrt(spread + norm_floor) * gain


def output_kernel(outer, place, rate, scaled, inner, token_scaled, token_key, token_value, gain, *refs):
    pieces, (mixed, new_read, parts, reads, sums) = refs[:PLANE], refs[PLANE:]
    step = pl.program_id(0)
    count, width = scaled.shape
    block = width // HEAD
    heads = sums.shape[0]
    held = HEAD // PLANE

    @pl.when(step == 0)
    def _():
        for r in range(PLANE):
            reads[place[1 + r]] = pieces[r][pl.ds(heads * held, 2 * heads), :].astype(f32)
        total = reads[0]
        for member in range(1, PLANE):
            total = total + reads[member]
        sums[...] = total[:heads] + total[heads:]

    offsets = lax.broadcasted_iota(jnp.int32, (count, HEAD), 0).astype(f32)
    for lane in range(block):
        columns = slice(lane * HEAD, (lane + 1) * HEAD)
        head = step * block + lane
        head_rate = rate[head]
        for r in range(PLANE):
            parts[place[1 + r]] = pieces[r][pl.ds(pl.multiple_of(head * held, held), held), :].astype(f32)
        split = [parts[member].reshape(outer, 1, held // outer, HEAD) for member in range(PLANE)]
        incoming = jnp.concatenate(split, axis=1).reshape(HEAD, HEAD).astype(bf16)
        carried = jnp.dot(scaled[:, columns], incoming, preferred_element_type=f32)
        gamma = jnp.exp(jnp.full((1, HEAD), -head_rate, f32))
        rows = (inner[:, columns] + carried * gamma) * jnp.exp(offsets * -head_rate)
        mixed[:, columns] = finish(rows, gain[:, columns]).astype(bf16)
        query = token_scaled[:, columns].astype(f32)[:1]
        key = token_key[:, columns].astype(f32)[:1]
        value = token_value[:, columns].astype(f32)[:1]
        own_score = jnp.sum(query * key, axis=-1, keepdims=True)
        read = gamma * sums[pl.ds(head, 1), :] + own_score * value
        new_read[:, columns] = finish(read, gain[:, columns]).astype(bf16)


def per_device(prompt, new_token, w_query, w_key, w_value, decay_rate, norm_gain):
    members = lax.axis_size("sp")
    heads = w_query.shape[1] // HEAD
    sequences, count, part = prompt.shape
    if (lax.axis_size("tp") != 2 or members % PLANE or HEAD % (8 * members) or sequences != 1 or heads % 8
            or count % 256 or count > 1024):
        return plain_device(prompt, new_token, w_query, w_key, w_value, decay_rate, norm_gain)
    outer = members // PLANE
    held = HEAD // PLANE
    features = 2 * part
    block = 2
    wide = block * HEAD
    width = heads * HEAD
    steps = heads // block
    rank = lax.axis_index("sp")
    member, line_rank = rank % PLANE, rank // PLANE
    place = jnp.stack([lax.axis_index("tp")] + [member ^ r for r in range(PLANE)]).astype(jnp.int32)
    line = jnp.stack([line_rank ^ s for s in range(outer)]).astype(jnp.int32)
    own = prompt.reshape(count, part)
    swap = [(0, 1), (1, 0)]
    other = lax.ppermute(own, "tp", swap)
    token_other = lax.ppermute(new_token, "tp", swap)

    lane = jnp.arange(HEAD, dtype=jnp.int32)
    inverse = rope_base ** (-(2 * (lane % (HEAD // 2))).astype(f32) / HEAD)
    index = jnp.arange(count + TOKEN_ROWS, dtype=jnp.int32)
    positions = jnp.where(index < count, rank * count + index, members * count)
    angles = positions.astype(f32)[:, None] * inverse[None, :]
    cosine = jnp.cos(angles)
    sine = jnp.sin(angles) * jnp.where(lane < HEAD // 2, -1.0, 1.0)[None, :]

    total_rows = count + TOKEN_ROWS
    column = pl.BlockSpec((count, wide), lambda i: (0, i))
    token_column = pl.BlockSpec((TOKEN_ROWS, wide), lambda i: (0, i))
    weight_column = pl.BlockSpec((features, wide), lambda i: (0, i))
    piece = pl.BlockSpec((block, held, HEAD), lambda i: (i, 0, 0))
    row_scratch = [pltpu.VMEM((total_rows, features), bf16), pltpu.VMEM((PLANE, held, HEAD), f32), pltpu.SemaphoreType.DMA((2,))]

    turned, values, token_key, token_value, *pieces = pl.pallas_call(
        lambda *refs: key_value_kernel(outer, *refs),
        grid=(steps,),
        in_specs=[smem(), smem(), hbm(), hbm(), vmem(), vmem(), weight_column, weight_column, vmem(), vmem()],
        out_specs=[column, column, token_column, token_column] + [piece] * PLANE,
        out_shape=[shape((count, width), bf16)] * 2 + [shape((TOKEN_ROWS, width), bf16)] * 2
        + [shape((heads, held, HEAD), bf16)] * PLANE,
        scratch_shapes=row_scratch,
        compiler_params=params(),
        name="key_value",
    )(place, decay_rate, own, other, new_token, token_other, w_key, w_value, cosine, sine)

    def plane_swap(items):
        return [items[0]] + [
            lax.ppermute(items[r], "sp", [(s, s ^ r) for s in range(members)]) for r in range(1, PLANE)
        ]

    gathered = plane_swap(pieces)

    scaled, token_scaled, token_rows = pl.pallas_call(
        lambda *refs: query_kernel(outer, *refs),
        grid=(steps,),
        in_specs=[smem(), hbm(), hbm(), vmem(), vmem(), weight_column, vmem(), vmem()],
        out_specs=[column, token_column, piece],
        out_shape=[shape((count, width), bf16), shape((TOKEN_ROWS, width), bf16), shape((heads, held, HEAD), f32)],
        scratch_shapes=row_scratch,
        compiler_params=params(),
        cost_estimate=pl.CostEstimate(flops=2 * total_rows * features * width, transcendentals=0, bytes_accessed=2 * features * width),
        name="query",
    )(place, own, other, new_token, token_other, w_query, cosine, sine)

    total, before = pl.pallas_call(
        lambda *refs: plane_kernel(count, *refs),
        in_specs=[smem(), smem()] + [vmem()] * PLANE,
        out_specs=[vmem(), vmem()],
        out_shape=[shape((heads, held, HEAD), bf16), shape((PLANE, heads, held, HEAD), f32)],
        scratch_shapes=[pltpu.VMEM((PLANE, heads, held, HEAD), f32)],
        compiler_params=params(),
        name="plane",
    )(place, decay_rate, *gathered)

    totals = [total] + [
        lax.ppermute(total, "sp", [(s, s ^ (PLANE * r)) for s in range(members)]) for r in range(1, outer)
    ]

    inner = pl.pallas_call(
        inner_kernel,
        grid=(steps,),
        in_specs=[smem(), column, column, column],
        out_specs=column,
        out_shape=shape((count, width), f32),
        compiler_params=params(),
        cost_estimate=pl.CostEstimate(flops=4 * count * count * width, transcendentals=0, bytes_accessed=10 * count * width),
        name="inner",
    )(decay_rate, scaled, turned, values)

    *results, cache = pl.pallas_call(
        lambda *refs: line_kernel(count, outer, *refs),
        in_specs=[smem(), smem(), smem()] + [vmem()] * (outer + 2),
        out_specs=[vmem()] * (PLANE + 1),
        out_shape=[shape((heads * held + 2 * heads, HEAD), bf16)] * PLANE + [shape((heads, held // outer, HEAD), bf16)],
        scratch_shapes=[
            pltpu.VMEM((outer, heads, held, HEAD), f32),
            pltpu.VMEM((outer, held, HEAD), f32),
            pltpu.VMEM((outer, held // outer, HEAD), f32),
            pltpu.VMEM((2 * heads, HEAD), f32),
        ],
        compiler_params=params(),
        name="line",
    )(place, line, decay_rate, *totals, before, token_rows)

    arrived = plane_swap(results)

    mixed, new_read = pl.pallas_call(
        lambda *refs: output_kernel(outer, *refs),
        grid=(steps,),
        in_specs=[smem(), smem(), column, column, token_column, token_column, token_column,
                  pl.BlockSpec((1, wide), lambda i: (0, i))] + [vmem()] * PLANE,
        out_specs=[column, pl.BlockSpec((1, wide), lambda i: (0, i))],
        out_shape=[shape((count, width), bf16), shape((1, width), bf16)],
        scratch_shapes=[
            pltpu.VMEM((PLANE, held, HEAD), f32),
            pltpu.VMEM((PLANE, 2 * heads, HEAD), f32),
            pltpu.VMEM((heads, HEAD), f32),
        ],
        compiler_params=params(),
        name="output",
    )(place, decay_rate, scaled, inner, token_scaled, token_key, token_value, norm_gain.reshape(1, width), *arrived)

    return (mixed.reshape(1, count, width), cache.reshape(1, heads, held // outer, HEAD), new_read)


def solution(mesh):
    in_specs = (
        P(None, "sp", "tp"),
        P(None, "tp"),
        P(None, "tp"),
        P(None, "tp"),
        P(None, "tp"),
        P("tp"),
        P("tp"),
    )
    out_specs = (P(None, "sp", "tp"), P(None, "tp", "sp", None), P(None, "tp"))
    return jax.shard_map(
        per_device, mesh=mesh, in_specs=in_specs, out_specs=out_specs, check_vma=False
    )
```

```python
import jax
import numpy as np
import jax.numpy as jnp
from jax import lax
from jax.experimental import pallas as pl
from jax.experimental.pallas import tpu as pltpu
from jax.sharding import PartitionSpec as P

HEAD = 128


rope_base = 10000.0
norm_floor = 1e-05


def rotate(tensor, positions):
    head_width = tensor.shape[-1]
    inverse = rope_base ** (-jnp.arange(0, head_width, 2, dtype=jnp.float32) / head_width)
    angles = positions.astype(jnp.float32)[:, None] * inverse[None, :]
    cosine = jnp.cos(angles)[:, None, :]
    sine_part = jnp.sin(angles)[:, None, :]
    first_half = tensor[..., : head_width // 2]
    second_half = tensor[..., head_width // 2 :]
    return jnp.concatenate(
        [
            first_half * cosine - second_half * sine_part,
            first_half * sine_part + second_half * cosine,
        ],
        axis=-1,
    )


def head_norm(output, gain):
    center = jnp.mean(output, axis=-1, keepdims=True)
    spread = jnp.mean(jnp.square(output - center), axis=-1, keepdims=True)
    return (output - center) * lax.rsqrt(spread + norm_floor) * gain


def decay_tables(log_gamma, block_size):
    offsets = jnp.arange(block_size, dtype=jnp.float32)
    gap_table = offsets[:, None] - offsets[None, :]
    within = jnp.where(
        gap_table[None] >= 0,
        jnp.exp(jnp.maximum(gap_table, 0.0)[None] * log_gamma[:, None, None]),
        0.0,
    )
    query_decay = jnp.exp((offsets[:, None] + 1.0) * log_gamma[None, :])
    key_decay = jnp.exp((block_size - 1.0 - offsets[:, None]) * log_gamma[None, :])
    return (within, query_decay, key_decay)


def plain_device(prompt, new_token, w_query, w_key, w_value, decay_rate, norm_gain):
    sequences, block_size, feature_part = prompt.shape
    head_count = w_query.shape[1] // HEAD
    members = lax.axis_size("sp")
    device_rank = lax.axis_index("sp")
    prompt_rows = sequences * block_size
    token_rows = jnp.concatenate([prompt.reshape(prompt_rows, feature_part), new_token], axis=0)
    weight_list = (w_query, w_key, w_value)
    shard_piece = lax.all_gather(token_rows, "tp", axis=1, tiled=True)
    projected = tuple(
        (jnp.dot(shard_piece, weight, preferred_element_type=jnp.float32) for weight in weight_list)
    )
    full_shape = (sequences, block_size, head_count, HEAD)
    queries, key_rows, values = [
        tensor[:prompt_rows].astype(jnp.bfloat16).reshape(full_shape) for tensor in projected
    ]
    token_query, token_key, token_value = [
        tensor[prompt_rows:].astype(jnp.bfloat16).reshape(sequences, 1, head_count, HEAD)
        for tensor in projected
    ]
    positions = device_rank * block_size + jnp.arange(block_size, dtype=jnp.int32)
    scaled = (rotate(queries.astype(jnp.float32), positions) * HEAD ** (-0.5)).astype(jnp.bfloat16)
    turned = rotate(key_rows.astype(jnp.float32), positions).astype(jnp.bfloat16)
    log_gamma = -decay_rate
    within, query_decay, key_decay = decay_tables(log_gamma, block_size)
    weighted = (turned.astype(jnp.float32) * key_decay[None, :, :, None]).astype(jnp.bfloat16)
    local_state = jnp.einsum(
        "smhd,smhe->shde", weighted, values, preferred_element_type=jnp.float32
    )
    pieces = lax.all_to_all(local_state[None], "sp", split_axis=3, concat_axis=0, tiled=True)
    source_index = jnp.arange(members, dtype=jnp.float32)
    gap_table = source_index[:, None] - 1.0 - source_index[None, :]
    weights = jnp.where(
        gap_table[None] >= 0,
        jnp.exp(jnp.maximum(gap_table, 0.0)[None] * block_size * log_gamma[:, None, None]),
        0.0,
    )
    prefix = jnp.einsum("hji,ishre->jshre", weights, pieces, precision=lax.Precision.HIGHEST)
    tail_all = jnp.exp((members - 1.0 - source_index)[None, :] * block_size * log_gamma[:, None])
    final_rows = jnp.einsum("hi,ishre->shre", tail_all, pieces, precision=lax.Precision.HIGHEST)
    incoming = lax.all_to_all(
        prefix.astype(jnp.bfloat16), "sp", split_axis=0, concat_axis=3, tiled=True
    ).astype(prefix.dtype)[0]
    scores = (
        jnp.einsum("snhd,smhd->shnm", scaled, turned, preferred_element_type=jnp.float32)
        * within[None]
    )
    inner_part = jnp.einsum(
        "shnm,smhe->snhe", scores.astype(jnp.bfloat16), values, preferred_element_type=jnp.float32
    )
    carried = (
        jnp.einsum(
            "snhd,shde->snhe",
            scaled,
            incoming.astype(jnp.bfloat16),
            preferred_element_type=jnp.float32,
        )
        * query_decay[None, :, :, None]
    )
    gain = norm_gain.reshape(head_count, HEAD)
    mixed = (
        head_norm(inner_part + carried, gain)
        .astype(jnp.bfloat16)
        .reshape(sequences, block_size, head_count * HEAD)
    )
    cache = final_rows.astype(jnp.bfloat16)
    token_positions = jnp.full((1,), block_size * members, jnp.int32)
    token_scaled = (
        rotate(token_query.astype(jnp.float32), token_positions) * HEAD ** (-0.5)
    ).astype(jnp.bfloat16)[:, 0]
    token_turned = rotate(token_key.astype(jnp.float32), token_positions).astype(jnp.bfloat16)[:, 0]
    row_count = final_rows.shape[2]
    query_rows = lax.dynamic_slice_in_dim(
        token_scaled, device_rank * row_count, row_count, 2
    ).astype(jnp.float32)
    partial_value = jnp.einsum(
        "shr,shre->she", query_rows, final_rows, precision=lax.Precision.HIGHEST
    )
    read_sum = lax.psum(partial_value, "sp")
    own_score = jnp.sum(
        token_scaled.astype(jnp.float32) * token_turned.astype(jnp.float32), axis=-1, keepdims=True
    )
    read_out = jnp.exp(log_gamma)[None, :, None] * read_sum + own_score * token_value[:, 0].astype(
        jnp.float32
    )
    new_read = head_norm(read_out, gain).astype(jnp.bfloat16).reshape(sequences, head_count * HEAD)
    return (mixed, cache, new_read)


PLANE = 4
TOKEN_ROWS = 16
WIDE = 2 * HEAD
f32 = jnp.float32
bf16 = jnp.bfloat16


def vmem():
    return pl.BlockSpec(memory_space=pltpu.VMEM)


def hbm():
    return pl.BlockSpec(memory_space=pltpu.HBM)


def anywhere():
    return pl.BlockSpec(memory_space=pl.ANY)


def far(array):
    return pltpu.with_memory_space_constraint(array, pltpu.HBM)


def params():
    return pltpu.CompilerParams(vmem_limit_bytes=24 * 1024 * 1024)


def cost(flops):
    return pl.CostEstimate(flops=int(flops), transcendentals=0, bytes_accessed=1 << 20)


def place():
    rank = lax.axis_index("sp")
    return rank % PLANE, rank // PLANE


def angle_tables(count, members):
    lane = np.arange(HEAD)
    inverse = rope_base ** (-2.0 * (lane % (HEAD // 2)) / HEAD)
    near = np.arange(count)[:, None] * inverse
    starts = (np.arange(members + 1) * count)[:, None] * inverse
    return [np.float32(f(angles)) for angles in (near, starts) for f in (np.cos, np.sin)]


def own_kernel(own, token_own, w_key, w_value, rate, near_cos, near_sin, start_cos, start_sin,
               rows, partial, key_rest, value_rest, cosine, sine, rates,
               weights, token, angles, scalars, sems):
    count, part = own.shape
    width = w_key.shape[1]
    chunks = width // WIDE
    near = pl.ds(pl.multiple_of(lax.axis_index("tp") * part, part), part)
    rest = pl.ds(pl.multiple_of((1 - lax.axis_index("tp")) * part, part), part)
    copies = [pltpu.make_async_copy(own, rows.at[pl.ds(0, count), :], sems.at[0])]
    copies.append(pltpu.make_async_copy(token_own, token, sems.at[1]))
    for index, matrix in enumerate((w_key, w_value)):
        for chunk in range(chunks):
            columns = pl.ds(chunk * WIDE, WIDE)
            copies.append(pltpu.make_async_copy(matrix.at[near, columns], weights.at[index, :, columns], sems.at[len(copies)]))
    late = len(copies)
    copies.append(pltpu.make_async_copy(near_cos, angles.at[0], sems.at[late]))
    copies.append(pltpu.make_async_copy(near_sin, angles.at[1], sems.at[late + 1]))
    copies.append(pltpu.make_async_copy(rate, scalars, sems.at[late + 2]))
    copies.append(pltpu.make_async_copy(w_key.at[rest, :], key_rest, sems.at[late + 3]))
    copies.append(pltpu.make_async_copy(w_value.at[rest, :], value_rest, sems.at[late + 4]))
    for copy in copies:
        copy.start()
    copies[0].wait()
    copies[1].wait()
    rows[pl.ds(count, TOKEN_ROWS), :] = jnp.broadcast_to(token[...], (TOKEN_ROWS, part))
    for index in range(2):
        for chunk in range(chunks):
            columns = slice(chunk * WIDE, (chunk + 1) * WIDE)
            copies[2 + index * chunks + chunk].wait()
            partial[:, index * width + chunk * WIDE:index * width + (chunk + 1) * WIDE] = jnp.dot(
                rows[...], weights[index, :, columns], preferred_element_type=f32)
    for copy in copies[late:late + 3]:
        copy.wait()
    rank = lax.axis_index("sp")
    last = start_cos.shape[0] - 1
    sign = jnp.where(lax.broadcasted_iota(jnp.int32, (1, HEAD), 1) < HEAD // 2, -1.0, 1.0)
    base_cos, base_sin = start_cos[pl.ds(rank, 1), :], start_sin[pl.ds(rank, 1), :]
    cosine[pl.ds(0, count), :] = angles[0] * base_cos - angles[1] * base_sin
    sine[pl.ds(0, count), :] = (angles[1] * base_cos + angles[0] * base_sin) * sign
    tail = (TOKEN_ROWS, HEAD)
    cosine[pl.ds(count, TOKEN_ROWS), :] = jnp.broadcast_to(start_cos[last:, :], tail)
    sine[pl.ds(count, TOKEN_ROWS), :] = jnp.broadcast_to(start_sin[last:, :] * sign, tail)
    for head in range(rates.shape[0]):
        rates[head:head + 1, :] = jnp.full((1, HEAD), scalars[head], f32)
    for copy in copies[late + 3:]:
        copy.wait()


def turn(rows, cosine, sine):
    return rows * cosine + pltpu.roll(rows, HEAD // 2, axis=1) * sine


def into_parts(matrix, parts, outer):
    rest = HEAD // (outer * PLANE)
    split = matrix.reshape(outer, PLANE, rest, HEAD)
    for member in range(PLANE):
        parts[member] = split[:, member].reshape(outer * rest, HEAD)


def key_value_kernel(outer, other, token_other, partial, key_rest, value_rest, cosine, sine, rates, w_query,
                     rows, turned, values, token_key, token_value, query_weights, *tail):
    pieces, (parts, sems) = tail[:PLANE], tail[PLANE:]
    member, _ = place()
    count, part = other.shape
    width = key_rest.shape[1]
    own = pl.ds(pl.multiple_of(lax.axis_index("tp") * part, part), part)
    rest = pl.ds(pl.multiple_of((1 - lax.axis_index("tp")) * part, part), part)
    first = pltpu.make_async_copy(w_query.at[own, :], query_weights.at[0], sems.at[0])
    second = pltpu.make_async_copy(w_query.at[rest, :], query_weights.at[1], sems.at[1])
    first.start()
    second.start()
    rows[pl.ds(0, count), :] = other[...]
    rows[pl.ds(count, TOKEN_ROWS), :] = jnp.broadcast_to(token_other[...], (TOKEN_ROWS, part))
    offsets = lax.broadcasted_iota(jnp.int32, (count, HEAD), 0).astype(f32)
    for chunk in range(width // WIDE):
        wide = slice(chunk * WIDE, (chunk + 1) * WIDE)
        key_rows = partial[:, wide] + jnp.dot(rows[...], key_rest[:, wide], preferred_element_type=f32)
        key_rows = key_rows.astype(bf16).astype(f32)
        value_rows = partial[:, width + chunk * WIDE:width + (chunk + 1) * WIDE] + jnp.dot(
            rows[...], value_rest[:, wide], preferred_element_type=f32)
        value_rows = value_rows.astype(bf16)
        values[:, wide] = value_rows[:count]
        token_value[:, wide] = value_rows[count:]
        for lane in range(WIDE // HEAD):
            head = chunk * (WIDE // HEAD) + lane
            inside = slice(lane * HEAD, (lane + 1) * HEAD)
            columns = slice(head * HEAD, (head + 1) * HEAD)
            result = turn(key_rows[:, inside], cosine[...], sine[...]).astype(bf16)
            turned[:, columns] = result[:count]
            token_key[:, columns] = result[count:]
            decay = jnp.exp((offsets - (count - 1.0)) * rates[head:head + 1, :])
            weighted = (result[:count].astype(f32) * decay).astype(bf16)
            local = lax.dot_general(weighted, value_rows[:count, inside], (((0,), (0,)), ((), ())), preferred_element_type=f32)
            into_parts(local, parts.at[head], outer)
            for r in range(PLANE):
                pieces[r][head] = parts[head, member ^ r].astype(bf16)
    first.wait()
    second.wait()


def query_kernel(outer, own_rows, other_rows, query_weights, cosine, sine, scaled, token_scaled, token_rows, parts):
    member, _ = place()
    count, width = scaled.shape
    for chunk in range(width // WIDE):
        wide = slice(chunk * WIDE, (chunk + 1) * WIDE)
        queries = jnp.dot(own_rows[...], query_weights[0, :, wide], preferred_element_type=f32) + jnp.dot(
            other_rows[...], query_weights[1, :, wide], preferred_element_type=f32)
        queries = queries.astype(bf16).astype(f32)
        for lane in range(WIDE // HEAD):
            head = chunk * (WIDE // HEAD) + lane
            inside = slice(lane * HEAD, (lane + 1) * HEAD)
            columns = slice(head * HEAD, (head + 1) * HEAD)
            result = (turn(queries[:, inside], cosine[...], sine[...]) * HEAD ** (-0.5)).astype(bf16)
            scaled[:, columns] = result[:count]
            token_scaled[:, columns] = result[count:]
            token = jnp.broadcast_to(result[count:].astype(f32)[:1], (HEAD, HEAD))
            into_parts(token.T, parts, outer)
            token_rows[head] = parts[member]


def inner_kernel(rates, scaled, turned, values, inner):
    count, width = scaled.shape
    half = count // 2
    lanes = lax.broadcasted_iota(jnp.int32, (1, count), 1).astype(f32)
    keep = lax.broadcasted_iota(jnp.int32, (half, half), 0) >= lax.broadcasted_iota(jnp.int32, (half, half), 1)
    for head in range(width // HEAD):
        columns = slice(head * HEAD, (head + 1) * HEAD)
        growth = jnp.exp(lanes * rates[head:head + 1, :1])

        def products(n, m):
            raw = lax.dot_general(scaled[n * half:(n + 1) * half, columns], turned[m * half:(m + 1) * half, columns],
                                  (((1,), (1,)), ((), ())), preferred_element_type=f32)
            raw = raw * growth[:, m * half:(m + 1) * half]
            return (jnp.where(keep, raw, 0.0) if n == m else raw).astype(bf16)

        low, high = values[:half, columns], values[half:, columns]
        inner[:half, columns] = jnp.dot(products(0, 0), low, preferred_element_type=f32)
        inner[half:, columns] = jnp.dot(products(1, 0), low, preferred_element_type=f32) + jnp.dot(
            products(1, 1), high, preferred_element_type=f32)


def plane_kernel(count, _, rates, *refs):
    pieces, (total, before, parts) = refs[:PLANE], refs[PLANE:]
    member, _ = place()
    for r in range(PLANE):
        parts[member ^ r] = pieces[r][...].astype(f32)
    for head in range(total.shape[0]):
        factor = jnp.exp(rates[head:head + 1, :] * -count)
        state = jnp.zeros(total.shape[1:], f32)
        for source in range(PLANE):
            before[source, head] = state
            state = state * factor + parts[source, head]
        total[head] = state.astype(bf16)


def line_kernel(count, outer, _, rates, *refs):
    totals = refs[:outer]
    before, token_rows = refs[outer:outer + 2]
    results, cache = refs[outer + 2:outer + 2 + PLANE], refs[outer + 2 + PLANE]
    ordered, running, final, reads = refs[outer + 3 + PLANE:]
    member, line = place()
    heads, width = totals[0].shape[:2]
    for s in range(outer):
        ordered[line ^ s] = totals[s][...].astype(f32)
    for head in range(heads):
        log_factor = rates[head:head + 1, :] * -count
        factor = jnp.exp(log_factor * PLANE)
        state = jnp.zeros((width, HEAD), f32)
        for source in range(outer):
            running[head, source] = state
            state = state * factor + ordered[source, head]
        final[head] = state.reshape(final.shape[1:])
        cache[head] = final[head, line].astype(bf16)
        read = jnp.sum(token_rows[head] * state, axis=0, keepdims=True)
        high = read.astype(bf16).astype(f32)
        reads[head:head + 1, :] = high
        reads[heads + head:heads + head + 1, :] = read - high
        arriving = running[head, line]
        for r in range(PLANE):
            scale = jnp.exp(log_factor * (member ^ r).astype(f32))
            results[r][pl.ds(head * width, width), :] = (before[member ^ r, head] + scale * arriving).astype(bf16)
    for r in range(PLANE):
        results[r][pl.ds(heads * width, 2 * heads), :] = reads[...].astype(bf16)


def finish(rows, gain):
    center = jnp.mean(rows, axis=-1, keepdims=True)
    rows = rows - center
    spread = jnp.mean(jnp.square(rows), axis=-1, keepdims=True)
    return rows * lax.rsqrt(spread + norm_floor) * gain


def output_kernel(outer, rates, scaled, inner, token_scaled, token_key, token_value, gain, *refs):
    pieces, (mixed, new_read, parts, reads, buffer, sems) = refs[:PLANE], refs[PLANE:]
    member, _ = place()
    count, width = scaled.shape
    heads = width // HEAD
    held = HEAD // PLANE
    for r in range(PLANE):
        parts[member ^ r] = pieces[r][pl.ds(0, heads * held), :].astype(f32)
        reads[member ^ r] = pieces[r][pl.ds(heads * held, 2 * heads), :].astype(f32)
    sums = reads[0]
    for source in range(1, PLANE):
        sums = sums + reads[source]
    sums = sums[:heads] + sums[heads:]
    offsets = lax.broadcasted_iota(jnp.int32, (count, HEAD), 0).astype(f32)
    copies = []
    for head in range(heads):
        columns = slice(head * HEAD, (head + 1) * HEAD)
        head_rate = -rates[head:head + 1, :]
        split = [parts[source, pl.ds(head * held, held), :].reshape(outer, 1, held // outer, HEAD) for source in range(PLANE)]
        incoming = jnp.concatenate(split, axis=1).reshape(HEAD, HEAD).astype(bf16)
        carried = jnp.dot(scaled[:, columns], incoming, preferred_element_type=f32)
        gamma = jnp.exp(head_rate)
        rows = (inner[:, columns] + carried * gamma) * jnp.exp(offsets * head_rate)
        buffer[:, columns] = finish(rows, gain[:, columns]).astype(bf16)
        query = token_scaled[:, columns].astype(f32)[:1]
        key = token_key[:, columns].astype(f32)[:1]
        value = token_value[:, columns].astype(f32)[:1]
        own_score = jnp.sum(query * key, axis=-1, keepdims=True)
        read = gamma * sums[head:head + 1] + own_score * value
        new_read[:, columns] = finish(read, gain[:, columns]).astype(bf16)
        if head % 2:
            wide = pl.ds((head - 1) * HEAD, WIDE)
            copies.append(pltpu.make_async_copy(buffer.at[:, wide], mixed.at[:, wide], sems.at[head // 2]))
            copies[-1].start()
    for copy in copies:
        copy.wait()


def per_device(prompt, new_token, w_query, w_key, w_value, decay_rate, norm_gain):
    members = lax.axis_size("sp")
    heads = w_query.shape[1] // HEAD
    sequences, count, part = prompt.shape
    if (lax.axis_size("tp") != 2 or members % PLANE or HEAD % (8 * members) or sequences != 1 or heads % 8
            or count % 256 or count > 1024):
        return plain_device(prompt, new_token, w_query, w_key, w_value, decay_rate, norm_gain)
    outer = members // PLANE
    held = HEAD // PLANE
    width = heads * HEAD
    total_rows = count + TOKEN_ROWS
    own = prompt.reshape(count, part)
    swap = [(0, 1), (1, 0)]
    other = lax.ppermute(own, "tp", swap)
    token_other = lax.ppermute(new_token, "tp", swap)
    dma = pltpu.SemaphoreType.DMA

    def call(kernel, name, arguments, specs, outs, out_specs, scratch, flops):
        return pl.pallas_call(kernel, in_specs=specs, out_specs=out_specs, out_shape=outs, scratch_shapes=scratch,
                              compiler_params=params(), cost_estimate=cost(flops), name=name)(*arguments)

    near_cos, near_sin, start_cos, start_sin = [jnp.asarray(t) for t in angle_tables(count, members)]
    rows, partial, key_rest, value_rest, cosine, sine, rates = call(
        own_kernel, "own",
        (far(own), far(new_token), far(w_key), far(w_value), far(decay_rate), far(near_cos), far(near_sin), start_cos, start_sin),
        [hbm()] * 7 + [vmem()] * 2,
        [pltpu.VMEM((total_rows, part), bf16), pltpu.VMEM((total_rows, 2 * width), f32), pltpu.VMEM((part, width), bf16),
         pltpu.VMEM((part, width), bf16), pltpu.VMEM((total_rows, HEAD), f32), pltpu.VMEM((total_rows, HEAD), f32),
         pltpu.VMEM((heads, HEAD), f32)],
        [vmem()] * 7,
        [pltpu.VMEM((2, part, width), bf16), pltpu.VMEM((1, part), bf16), pltpu.VMEM((2, count, HEAD), f32),
         pltpu.SMEM((heads,), f32), dma((7 + 2 * width // WIDE,))],
        4 * total_rows * part * width)

    other_rows, turned, values, token_key, token_value, query_weights, *pieces = call(
        lambda *refs: key_value_kernel(outer, *refs), "key_value",
        (other, token_other, partial, key_rest, value_rest, cosine, sine, rates, far(w_query)),
        [vmem()] * 8 + [hbm()],
        [pltpu.VMEM((total_rows, part), bf16), pltpu.VMEM((count, width), bf16), pltpu.VMEM((count, width), bf16),
         pltpu.VMEM((TOKEN_ROWS, width), bf16), pltpu.VMEM((TOKEN_ROWS, width), bf16), pltpu.VMEM((2, part, width), bf16)]
        + [pltpu.VMEM((heads, held, HEAD), bf16)] * PLANE,
        [vmem()] * (6 + PLANE),
        [pltpu.VMEM((heads, PLANE, held, HEAD), f32), dma((2,))],
        4 * total_rows * part * width)

    def plane_swap(items):
        return [items[0]] + [
            lax.ppermute(items[r], "sp", [(s, s ^ r) for s in range(members)]) for r in range(1, PLANE)
        ]

    gathered = plane_swap(pieces)

    scaled, token_scaled, token_rows = call(
        lambda *refs: query_kernel(outer, *refs), "query",
        (rows, other_rows, query_weights, cosine, sine),
        [vmem()] * 5,
        [pltpu.VMEM((count, width), bf16), pltpu.VMEM((TOKEN_ROWS, width), bf16), pltpu.VMEM((heads, held, HEAD), f32)],
        [vmem()] * 3,
        [pltpu.VMEM((PLANE, held, HEAD), f32)],
        4 * total_rows * part * width)

    total, before = call(
        lambda *refs: plane_kernel(count, *refs), "plane",
        (token_scaled, rates, *gathered),
        [anywhere()] + [vmem()] * (1 + PLANE),
        [pltpu.VMEM((heads, held, HEAD), bf16), pltpu.VMEM((PLANE, heads, held, HEAD), f32)],
        [vmem()] * 2,
        [pltpu.VMEM((PLANE, heads, held, HEAD), f32)],
        1 << 20)

    totals = [total] + [
        lax.ppermute(total, "sp", [(s, s ^ (PLANE * r)) for s in range(members)]) for r in range(1, outer)
    ]

    inner = call(
        inner_kernel, "inner",
        (rates, scaled, turned, values),
        [vmem()] * 4, pltpu.VMEM((count, width), f32), vmem(), [],
        4 * count * count * width)

    *results, cache = call(
        lambda *refs: line_kernel(count, outer, *refs), "line",
        (inner, rates, *totals, before, token_rows),
        [anywhere()] + [vmem()] * (outer + 3),
        [pltpu.VMEM((heads * held + 2 * heads, HEAD), bf16)] * PLANE + [shape((heads, held // outer, HEAD), bf16)],
        [vmem()] * (PLANE + 1),
        [pltpu.VMEM((outer, heads, held, HEAD), f32), pltpu.VMEM((heads, outer, held, HEAD), f32),
         pltpu.VMEM((heads, outer, held // outer, HEAD), f32), pltpu.VMEM((2 * heads, HEAD), f32)],
        1 << 20)

    arrived = plane_swap(results)

    mixed, new_read = call(
        lambda *refs: output_kernel(outer, *refs), "output",
        (rates, scaled, inner, token_scaled, token_key, token_value, norm_gain.reshape(1, width), *arrived),
        [vmem()] * (7 + PLANE),
        [shape((count, width), bf16), shape((1, width), bf16)],
        [hbm(), vmem()],
        [pltpu.VMEM((PLANE, heads * held, HEAD), f32), pltpu.VMEM((PLANE, 2 * heads, HEAD), f32),
         pltpu.VMEM((count, width), bf16), dma((heads // 2,))],
        1 << 20)

    return (mixed.reshape(1, count, width), cache.reshape(1, heads, held // outer, HEAD), new_read)


def shape(dims, dtype):
    return jax.ShapeDtypeStruct(dims, dtype)


def solution(mesh):
    in_specs = (
        P(None, "sp", "tp"),
        P(None, "tp"),
        P(None, "tp"),
        P(None, "tp"),
        P(None, "tp"),
        P("tp"),
        P("tp"),
    )
    out_specs = (P(None, "sp", "tp"), P(None, "tp", "sp", None), P(None, "tp"))
    return jax.shard_map(
        per_device, mesh=mesh, in_specs=in_specs, out_specs=out_specs, check_vma=False
    )
```

```python
import jax
import numpy as np
import jax.numpy as jnp
from jax import lax
from jax.experimental import pallas as pl
from jax.experimental.pallas import tpu as pltpu
from jax.sharding import PartitionSpec as P

HEAD = 128


rope_base = 10000.0
norm_floor = 1e-05


def rotate(tensor, positions):
    head_width = tensor.shape[-1]
    inverse = rope_base ** (-jnp.arange(0, head_width, 2, dtype=jnp.float32) / head_width)
    angles = positions.astype(jnp.float32)[:, None] * inverse[None, :]
    cosine = jnp.cos(angles)[:, None, :]
    sine_part = jnp.sin(angles)[:, None, :]
    first_half = tensor[..., : head_width // 2]
    second_half = tensor[..., head_width // 2 :]
    return jnp.concatenate(
        [
            first_half * cosine - second_half * sine_part,
            first_half * sine_part + second_half * cosine,
        ],
        axis=-1,
    )


def head_norm(output, gain):
    center = jnp.mean(output, axis=-1, keepdims=True)
    spread = jnp.mean(jnp.square(output - center), axis=-1, keepdims=True)
    return (output - center) * lax.rsqrt(spread + norm_floor) * gain


def decay_tables(log_gamma, block_size):
    offsets = jnp.arange(block_size, dtype=jnp.float32)
    gap_table = offsets[:, None] - offsets[None, :]
    within = jnp.where(
        gap_table[None] >= 0,
        jnp.exp(jnp.maximum(gap_table, 0.0)[None] * log_gamma[:, None, None]),
        0.0,
    )
    query_decay = jnp.exp((offsets[:, None] + 1.0) * log_gamma[None, :])
    key_decay = jnp.exp((block_size - 1.0 - offsets[:, None]) * log_gamma[None, :])
    return (within, query_decay, key_decay)


def plain_device(prompt, new_token, w_query, w_key, w_value, decay_rate, norm_gain):
    sequences, block_size, feature_part = prompt.shape
    head_count = w_query.shape[1] // HEAD
    members = lax.axis_size("sp")
    device_rank = lax.axis_index("sp")
    prompt_rows = sequences * block_size
    token_rows = jnp.concatenate([prompt.reshape(prompt_rows, feature_part), new_token], axis=0)
    weight_list = (w_query, w_key, w_value)
    shard_piece = lax.all_gather(token_rows, "tp", axis=1, tiled=True)
    projected = tuple(
        (jnp.dot(shard_piece, weight, preferred_element_type=jnp.float32) for weight in weight_list)
    )
    full_shape = (sequences, block_size, head_count, HEAD)
    queries, key_rows, values = [
        tensor[:prompt_rows].astype(jnp.bfloat16).reshape(full_shape) for tensor in projected
    ]
    token_query, token_key, token_value = [
        tensor[prompt_rows:].astype(jnp.bfloat16).reshape(sequences, 1, head_count, HEAD)
        for tensor in projected
    ]
    positions = device_rank * block_size + jnp.arange(block_size, dtype=jnp.int32)
    scaled = (rotate(queries.astype(jnp.float32), positions) * HEAD ** (-0.5)).astype(jnp.bfloat16)
    turned = rotate(key_rows.astype(jnp.float32), positions).astype(jnp.bfloat16)
    log_gamma = -decay_rate
    within, query_decay, key_decay = decay_tables(log_gamma, block_size)
    weighted = (turned.astype(jnp.float32) * key_decay[None, :, :, None]).astype(jnp.bfloat16)
    local_state = jnp.einsum(
        "smhd,smhe->shde", weighted, values, preferred_element_type=jnp.float32
    )
    pieces = lax.all_to_all(local_state[None], "sp", split_axis=3, concat_axis=0, tiled=True)
    source_index = jnp.arange(members, dtype=jnp.float32)
    gap_table = source_index[:, None] - 1.0 - source_index[None, :]
    weights = jnp.where(
        gap_table[None] >= 0,
        jnp.exp(jnp.maximum(gap_table, 0.0)[None] * block_size * log_gamma[:, None, None]),
        0.0,
    )
    prefix = jnp.einsum("hji,ishre->jshre", weights, pieces, precision=lax.Precision.HIGHEST)
    tail_all = jnp.exp((members - 1.0 - source_index)[None, :] * block_size * log_gamma[:, None])
    final_rows = jnp.einsum("hi,ishre->shre", tail_all, pieces, precision=lax.Precision.HIGHEST)
    incoming = lax.all_to_all(
        prefix.astype(jnp.bfloat16), "sp", split_axis=0, concat_axis=3, tiled=True
    ).astype(prefix.dtype)[0]
    scores = (
        jnp.einsum("snhd,smhd->shnm", scaled, turned, preferred_element_type=jnp.float32)
        * within[None]
    )
    inner_part = jnp.einsum(
        "shnm,smhe->snhe", scores.astype(jnp.bfloat16), values, preferred_element_type=jnp.float32
    )
    carried = (
        jnp.einsum(
            "snhd,shde->snhe",
            scaled,
            incoming.astype(jnp.bfloat16),
            preferred_element_type=jnp.float32,
        )
        * query_decay[None, :, :, None]
    )
    gain = norm_gain.reshape(head_count, HEAD)
    mixed = (
        head_norm(inner_part + carried, gain)
        .astype(jnp.bfloat16)
        .reshape(sequences, block_size, head_count * HEAD)
    )
    cache = final_rows.astype(jnp.bfloat16)
    token_positions = jnp.full((1,), block_size * members, jnp.int32)
    token_scaled = (
        rotate(token_query.astype(jnp.float32), token_positions) * HEAD ** (-0.5)
    ).astype(jnp.bfloat16)[:, 0]
    token_turned = rotate(token_key.astype(jnp.float32), token_positions).astype(jnp.bfloat16)[:, 0]
    row_count = final_rows.shape[2]
    query_rows = lax.dynamic_slice_in_dim(
        token_scaled, device_rank * row_count, row_count, 2
    ).astype(jnp.float32)
    partial_value = jnp.einsum(
        "shr,shre->she", query_rows, final_rows, precision=lax.Precision.HIGHEST
    )
    read_sum = lax.psum(partial_value, "sp")
    own_score = jnp.sum(
        token_scaled.astype(jnp.float32) * token_turned.astype(jnp.float32), axis=-1, keepdims=True
    )
    read_out = jnp.exp(log_gamma)[None, :, None] * read_sum + own_score * token_value[:, 0].astype(
        jnp.float32
    )
    new_read = head_norm(read_out, gain).astype(jnp.bfloat16).reshape(sequences, head_count * HEAD)
    return (mixed, cache, new_read)


PLANE = 4
TOKEN_ROWS = 16
WIDE = 2 * HEAD
BROAD = 4 * HEAD
f32 = jnp.float32
bf16 = jnp.bfloat16


def vmem():
    return pl.BlockSpec(memory_space=pltpu.VMEM)


def hbm():
    return pl.BlockSpec(memory_space=pltpu.HBM)


def anywhere():
    return pl.BlockSpec(memory_space=pl.ANY)


def far(array):
    return pltpu.with_memory_space_constraint(array, pltpu.HBM)


def params():
    return pltpu.CompilerParams(vmem_limit_bytes=24 * 1024 * 1024)


def cost(flops):
    return pl.CostEstimate(flops=int(flops), transcendentals=0, bytes_accessed=1 << 20)


def place():
    rank = lax.axis_index("sp")
    return rank % PLANE, rank // PLANE


def angle_tables(count, members):
    lane = np.arange(HEAD)
    inverse = rope_base ** (-2.0 * (lane % (HEAD // 2)) / HEAD)
    near = np.arange(count)[:, None] * inverse
    starts = (np.arange(members + 1) * count)[:, None] * inverse
    return [np.float32(f(angles)) for angles in (near, starts) for f in (np.cos, np.sin)]


def own_kernel(own, token_own, w_key, w_value, rate, near_cos, near_sin, starts,
               rows, partial, key_rest, cosine, sine, rates,
               weights, token, angles, bases, scalars, sems):
    count, part = own.shape
    width = w_key.shape[1]
    chunks = width // BROAD
    near = pl.ds(pl.multiple_of(lax.axis_index("tp") * part, part), part)
    rest = pl.ds(pl.multiple_of((1 - lax.axis_index("tp")) * part, part), part)
    copies = []

    def copy(source, target):
        copies.append(pltpu.make_async_copy(source, target, sems.at[len(copies)]))
        copies[-1].start()

    copy(token_own, token)
    copy(own, rows.at[pl.ds(0, count), :])
    for index, matrix in enumerate((w_key, w_value)):
        for chunk in range(chunks):
            columns = pl.ds(chunk * BROAD, BROAD)
            copy(matrix.at[near, columns], weights.at[index, :, columns])
    late = len(copies)
    copy(rate, scalars)
    copy(starts, bases)
    copy(near_cos, angles.at[0])
    copy(near_sin, angles.at[1])
    copy(w_key.at[rest, :], key_rest)
    copies[0].wait()
    copies[1].wait()
    rows[pl.ds(count, TOKEN_ROWS), :] = jnp.broadcast_to(token[...], (TOKEN_ROWS, part))
    for index in range(2):
        for chunk in range(chunks):
            columns = slice(chunk * BROAD, (chunk + 1) * BROAD)
            copies[2 + index * chunks + chunk].wait()
            if index == 1 and chunk == chunks - 1:
                for item in copies[late:-1]:
                    item.wait()
                rank = lax.axis_index("sp")
                last = starts.shape[1] - 1
                sign = jnp.where(lax.broadcasted_iota(jnp.int32, (1, HEAD), 1) < HEAD // 2, -1.0, 1.0)
                base_cos, base_sin = bases[0, pl.ds(rank, 1), :], bases[1, pl.ds(rank, 1), :]
                cosine[pl.ds(0, count), :] = angles[0] * base_cos - angles[1] * base_sin
                sine[pl.ds(0, count), :] = (angles[1] * base_cos + angles[0] * base_sin) * sign
                tail = (TOKEN_ROWS, HEAD)
                cosine[pl.ds(count, TOKEN_ROWS), :] = jnp.broadcast_to(bases[0, last:, :], tail)
                sine[pl.ds(count, TOKEN_ROWS), :] = jnp.broadcast_to(bases[1, last:, :] * sign, tail)
                for head in range(rates.shape[0]):
                    rates[head:head + 1, :] = jnp.full((1, HEAD), scalars[head], f32)
            partial[:, index * width + chunk * BROAD:index * width + (chunk + 1) * BROAD] = jnp.dot(
                rows[...], weights[index, :, columns], preferred_element_type=f32)
    copies[-1].wait()


def turn(rows, cosine, sine):
    return rows * cosine + pltpu.roll(rows, HEAD // 2, axis=1) * sine


def into_parts(matrix, parts, outer):
    rest = HEAD // (outer * PLANE)
    split = matrix.reshape(outer, PLANE, rest, HEAD)
    for member in range(PLANE):
        parts[member] = split[:, member].reshape(outer * rest, HEAD)


def key_value_kernel(outer, other, token_other, partial, key_rest, cosine, sine, rates, w_value, w_query,
                     rows, turned, values, token_key, token_value, query_weights, *tail):
    pieces, (value_rest, weighted, parts, sems) = tail[:PLANE], tail[PLANE:]
    member, _ = place()
    count, part = other.shape
    width = key_rest.shape[1]
    own = pl.ds(pl.multiple_of(lax.axis_index("tp") * part, part), part)
    rest = pl.ds(pl.multiple_of((1 - lax.axis_index("tp")) * part, part), part)
    third = pltpu.make_async_copy(w_value.at[rest, :], value_rest, sems.at[2])
    first = pltpu.make_async_copy(w_query.at[own, :], query_weights.at[0], sems.at[0])
    second = pltpu.make_async_copy(w_query.at[rest, :], query_weights.at[1], sems.at[1])
    third.start()
    first.start()
    second.start()
    rows[pl.ds(0, count), :] = other[...]
    rows[pl.ds(count, TOKEN_ROWS), :] = jnp.broadcast_to(token_other[...], (TOKEN_ROWS, part))
    offsets = lax.broadcasted_iota(jnp.int32, (count, HEAD), 0).astype(f32)
    lanes = BROAD // HEAD
    for chunk in range(width // BROAD):
        broad = slice(chunk * BROAD, (chunk + 1) * BROAD)
        key_rows = partial[:, broad] + jnp.dot(rows[...], key_rest[:, broad], preferred_element_type=f32)
        key_rows = key_rows.astype(bf16).astype(f32)
        for lane in range(lanes):
            head = chunk * lanes + lane
            inside = slice(lane * HEAD, (lane + 1) * HEAD)
            columns = slice(head * HEAD, (head + 1) * HEAD)
            result = turn(key_rows[:, inside], cosine[...], sine[...]).astype(bf16)
            turned[:, columns] = result[:count]
            token_key[:, columns] = result[count:]
            decay = jnp.exp((offsets - (count - 1.0)) * rates[head:head + 1, :])
            weighted[:, columns] = (result[:count].astype(f32) * decay).astype(bf16)
    third.wait()
    for chunk in range(width // BROAD):
        broad = slice(chunk * BROAD, (chunk + 1) * BROAD)
        value_rows = partial[:, width + chunk * BROAD:width + (chunk + 1) * BROAD] + jnp.dot(
            rows[...], value_rest[:, broad], preferred_element_type=f32)
        value_rows = value_rows.astype(bf16)
        values[:, broad] = value_rows[:count]
        token_value[:, broad] = value_rows[count:]
        for lane in range(lanes):
            head = chunk * lanes + lane
            inside = slice(lane * HEAD, (lane + 1) * HEAD)
            columns = slice(head * HEAD, (head + 1) * HEAD)
            local = lax.dot_general(weighted[:, columns], value_rows[:count, inside], (((0,), (0,)), ((), ())),
                                    preferred_element_type=f32)
            into_parts(local, parts.at[head], outer)
            for r in range(PLANE):
                pieces[r][head] = parts[head, member ^ r].astype(bf16)
    first.wait()
    second.wait()


def query_kernel(outer, own_rows, other_rows, query_weights, cosine, sine, scaled, token_scaled, token_rows, parts):
    member, _ = place()
    count, width = scaled.shape
    for chunk in range(width // BROAD):
        wide = slice(chunk * BROAD, (chunk + 1) * BROAD)
        queries = jnp.dot(own_rows[...], query_weights[0, :, wide], preferred_element_type=f32) + jnp.dot(
            other_rows[...], query_weights[1, :, wide], preferred_element_type=f32)
        queries = queries.astype(bf16).astype(f32)
        for lane in range(BROAD // HEAD):
            head = chunk * (BROAD // HEAD) + lane
            inside = slice(lane * HEAD, (lane + 1) * HEAD)
            columns = slice(head * HEAD, (head + 1) * HEAD)
            result = (turn(queries[:, inside], cosine[...], sine[...]) * HEAD ** (-0.5)).astype(bf16)
            scaled[:, columns] = result[:count]
            token_scaled[:, columns] = result[count:]
            token = jnp.broadcast_to(result[count:].astype(f32)[:1], (HEAD, HEAD))
            into_parts(token.T, parts.at[head], outer)
            token_rows[head] = parts[head, member]


def inner_kernel(start, rates, scaled, turned, values, _, inner, fade):
    count, width = inner.shape
    half = count // 2
    lanes = lax.broadcasted_iota(jnp.int32, (1, count), 1).astype(f32)
    offsets = lax.broadcasted_iota(jnp.int32, (count, HEAD), 0).astype(f32)
    keep = lax.broadcasted_iota(jnp.int32, (half, half), 0) >= lax.broadcasted_iota(jnp.int32, (half, half), 1)
    for index in range(width // HEAD):
        head = start + index
        columns = slice(head * HEAD, (head + 1) * HEAD)
        place_in = slice(index * HEAD, (index + 1) * HEAD)
        growth = jnp.exp(lanes * rates[head:head + 1, :1])
        decay = jnp.exp(-offsets * rates[head:head + 1, :])
        fade[:, place_in] = decay * jnp.exp(-rates[head:head + 1, :])

        def products(n, m):
            raw = lax.dot_general(scaled[n * half:(n + 1) * half, columns], turned[m * half:(m + 1) * half, columns],
                                  (((1,), (1,)), ((), ())), preferred_element_type=f32)
            raw = raw * growth[:, m * half:(m + 1) * half]
            return (jnp.where(keep, raw, 0.0) if n == m else raw).astype(bf16)

        low, high = values[:half, columns], values[half:, columns]
        inner[:half, place_in] = jnp.dot(products(0, 0), low, preferred_element_type=f32) * decay[:half]
        inner[half:, place_in] = (jnp.dot(products(1, 0), low, preferred_element_type=f32) + jnp.dot(
            products(1, 1), high, preferred_element_type=f32)) * decay[half:]


def plane_kernel(count, _, rates, *refs):
    pieces, (total, before, parts) = refs[:PLANE], refs[PLANE:]
    member, _ = place()
    for r in range(PLANE):
        parts[member ^ r] = pieces[r][...].astype(f32)
    for head in range(total.shape[0]):
        factor = jnp.exp(rates[head:head + 1, :] * -count)
        state = jnp.zeros(total.shape[1:], f32)
        for source in range(PLANE):
            before[source, head] = state
            state = state * factor + parts[source, head]
        total[head] = state.astype(bf16)


def line_kernel(count, outer, _, rates, *refs):
    totals = refs[:outer]
    before, token_rows = refs[outer:outer + 2]
    results, cache = refs[outer + 2:outer + 2 + PLANE], refs[outer + 2 + PLANE]
    ordered, running, final, reads = refs[outer + 3 + PLANE:]
    member, line = place()
    heads, width = totals[0].shape[:2]
    for s in range(outer):
        ordered[line ^ s] = totals[s][...].astype(f32)
    for head in range(heads):
        log_factor = rates[head:head + 1, :] * -count
        factor = jnp.exp(log_factor * PLANE)
        state = jnp.zeros((width, HEAD), f32)
        for source in range(outer):
            running[head, source] = state
            state = state * factor + ordered[source, head]
        final[head] = state.reshape(final.shape[1:])
        cache[head] = final[head, line].astype(bf16)
        read = jnp.sum(token_rows[head] * state, axis=0, keepdims=True)
        high = read.astype(bf16).astype(f32)
        reads[head:head + 1, :] = high
        reads[heads + head:heads + head + 1, :] = read - high
        arriving = running[head, line]
        for r in range(PLANE):
            scale = jnp.exp(log_factor * (member ^ r).astype(f32))
            results[r][pl.ds(head * width, width), :] = (before[member ^ r, head] + scale * arriving).astype(bf16)
    for r in range(PLANE):
        results[r][pl.ds(heads * width, 2 * heads), :] = reads[...].astype(bf16)


def finish(rows, gain):
    center = jnp.mean(rows, axis=-1, keepdims=True)
    rows = rows - center
    spread = jnp.mean(jnp.square(rows), axis=-1, keepdims=True)
    return rows * lax.rsqrt(spread + norm_floor) * gain


def output_kernel(outer, rates, scaled, inner_low, inner_high, fade_low, fade_high, token_scaled, token_key, token_value,
                  gain, *refs):
    pieces, (mixed, new_read, parts, reads, buffer, sems) = refs[:PLANE], refs[PLANE:]
    member, _ = place()
    count, width = scaled.shape
    heads = width // HEAD
    held = HEAD // PLANE
    for r in range(PLANE):
        parts[member ^ r] = pieces[r][pl.ds(0, heads * held), :].astype(f32)
        reads[member ^ r] = pieces[r][pl.ds(heads * held, 2 * heads), :].astype(f32)
    sums = reads[0]
    for source in range(1, PLANE):
        sums = sums + reads[source]
    sums = sums[:heads] + sums[heads:]
    rows_of = lax.broadcasted_iota(jnp.int32, (WIDE, WIDE), 0) // HEAD
    columns_of = lax.broadcasted_iota(jnp.int32, (WIDE, WIDE), 1) // HEAD
    average = jnp.where(rows_of == columns_of, 1.0 / HEAD, 0.0).astype(bf16)
    blank = jnp.zeros((HEAD, HEAD), bf16)

    def averaged(items):
        return jnp.dot(items, average, preferred_element_type=f32)

    copies = []
    for pair in range(heads // 2):
        wide = slice(pair * WIDE, (pair + 1) * WIDE)
        inner, fade = (inner_low, fade_low) if pair < heads // 4 else (inner_high, fade_high)
        inside = slice(pair % (heads // 4) * WIDE, (pair % (heads // 4) + 1) * WIDE)
        states = []
        for head in (2 * pair, 2 * pair + 1):
            split = [parts[source, pl.ds(head * held, held), :].reshape(outer, 1, held // outer, HEAD) for source in range(PLANE)]
            states.append(jnp.concatenate(split, axis=1).reshape(HEAD, HEAD).astype(bf16))
        incoming = jnp.concatenate([jnp.concatenate([states[0], blank], axis=1), jnp.concatenate([blank, states[1]], axis=1)], axis=0)
        carried = jnp.dot(scaled[:, wide], incoming, preferred_element_type=f32)
        rows = inner[:, inside] + carried * fade[:, inside]
        high = rows.astype(bf16)
        low = (rows - high.astype(f32)).astype(bf16)
        rows = rows - (averaged(high) + averaged(low))
        spread = averaged((rows * rows).astype(bf16))
        buffer[:, wide] = (rows * lax.rsqrt(spread + norm_floor) * gain[:, wide]).astype(bf16)
        copies.append(pltpu.make_async_copy(buffer.at[:, pl.ds(pair * WIDE, WIDE)], mixed.at[:, pl.ds(pair * WIDE, WIDE)], sems.at[pair]))
        copies[-1].start()
    for head in range(heads):
        columns = slice(head * HEAD, (head + 1) * HEAD)
        query = token_scaled[:, columns].astype(f32)[:1]
        key = token_key[:, columns].astype(f32)[:1]
        value = token_value[:, columns].astype(f32)[:1]
        own_score = jnp.sum(query * key, axis=-1, keepdims=True)
        read = jnp.exp(-rates[head:head + 1, :]) * sums[head:head + 1] + own_score * value
        new_read[:, columns] = finish(read, gain[:, columns]).astype(bf16)
    for copy in copies:
        copy.wait()


def per_device(prompt, new_token, w_query, w_key, w_value, decay_rate, norm_gain):
    members = lax.axis_size("sp")
    heads = w_query.shape[1] // HEAD
    sequences, count, part = prompt.shape
    if (lax.axis_size("tp") != 2 or members % PLANE or HEAD % (8 * members) or sequences != 1 or heads % 8
            or count % 256 or count > 1024):
        return plain_device(prompt, new_token, w_query, w_key, w_value, decay_rate, norm_gain)
    outer = members // PLANE
    held = HEAD // PLANE
    width = heads * HEAD
    total_rows = count + TOKEN_ROWS
    own = prompt.reshape(count, part)
    swap = [(0, 1), (1, 0)]
    other = lax.ppermute(own, "tp", swap)
    token_other = lax.ppermute(new_token, "tp", swap)
    dma = pltpu.SemaphoreType.DMA

    def call(kernel, name, arguments, specs, outs, out_specs, scratch, flops):
        return pl.pallas_call(kernel, in_specs=specs, out_specs=out_specs, out_shape=outs, scratch_shapes=scratch,
                              compiler_params=params(), cost_estimate=cost(flops), name=name)(*arguments)

    near_cos, near_sin, start_cos, start_sin = angle_tables(count, members)
    near_cos, near_sin, starts = jnp.asarray(near_cos), jnp.asarray(near_sin), jnp.asarray(np.stack([start_cos, start_sin]))
    rows, partial, key_rest, cosine, sine, rates = call(
        own_kernel, "own",
        (far(own), far(new_token), far(w_key), far(w_value), far(decay_rate), far(near_cos), far(near_sin), far(starts)),
        [hbm()] * 8,
        [pltpu.VMEM((total_rows, part), bf16), pltpu.VMEM((total_rows, 2 * width), f32), pltpu.VMEM((part, width), bf16),
         pltpu.VMEM((total_rows, HEAD), f32), pltpu.VMEM((total_rows, HEAD), f32), pltpu.VMEM((heads, HEAD), f32)],
        [vmem()] * 6,
        [pltpu.VMEM((2, part, width), bf16), pltpu.VMEM((1, part), bf16), pltpu.VMEM((2, count, HEAD), f32),
         pltpu.VMEM(starts.shape, f32), pltpu.SMEM((heads,), f32), dma((7 + 2 * width // BROAD,))],
        4 * total_rows * part * width)

    other_rows, turned, values, token_key, token_value, query_weights, *pieces = call(
        lambda *refs: key_value_kernel(outer, *refs), "key_value",
        (other, token_other, partial, key_rest, cosine, sine, rates, far(w_value), far(w_query)),
        [vmem()] * 7 + [hbm()] * 2,
        [pltpu.VMEM((total_rows, part), bf16), pltpu.VMEM((count, width), bf16), pltpu.VMEM((count, width), bf16),
         pltpu.VMEM((TOKEN_ROWS, width), bf16), pltpu.VMEM((TOKEN_ROWS, width), bf16), pltpu.VMEM((2, part, width), bf16)]
        + [pltpu.VMEM((heads, held, HEAD), bf16)] * PLANE,
        [vmem()] * (6 + PLANE),
        [pltpu.VMEM((part, width), bf16), pltpu.VMEM((count, width), bf16), pltpu.VMEM((heads, PLANE, held, HEAD), f32), dma((3,))],
        4 * total_rows * part * width)

    def plane_swap(items):
        return [items[0]] + [
            lax.ppermute(items[r], "sp", [(s, s ^ r) for s in range(members)]) for r in range(1, PLANE)
        ]

    gathered = plane_swap(pieces)

    scaled, token_scaled, token_rows = call(
        lambda *refs: query_kernel(outer, *refs), "query",
        (rows, other_rows, query_weights, cosine, sine),
        [vmem()] * 5,
        [pltpu.VMEM((count, width), bf16), pltpu.VMEM((TOKEN_ROWS, width), bf16), pltpu.VMEM((heads, held, HEAD), f32)],
        [vmem()] * 3,
        [pltpu.VMEM((heads, PLANE, held, HEAD), f32)],
        4 * total_rows * part * width)

    total, before = call(
        lambda *refs: plane_kernel(count, *refs), "plane",
        (token_scaled, rates, *gathered),
        [anywhere()] + [vmem()] * (1 + PLANE),
        [pltpu.VMEM((heads, held, HEAD), bf16), pltpu.VMEM((PLANE, heads, held, HEAD), f32)],
        [vmem()] * 2,
        [pltpu.VMEM((PLANE, heads, held, HEAD), f32)],
        1 << 20)

    totals = [total] + [
        lax.ppermute(total, "sp", [(s, s ^ (PLANE * r)) for s in range(members)]) for r in range(1, outer)
    ]

    def inside(start, name, after):
        return call(
            lambda *refs: inner_kernel(start, *refs), name,
            (rates, scaled, turned, values, after),
            [vmem()] * 4 + [anywhere()], [pltpu.VMEM((count, width // 2), f32)] * 2, [vmem()] * 2, [],
            2 * count * count * width)

    inner_low, fade_low = inside(0, "inner_low", total)

    *results, cache = call(
        lambda *refs: line_kernel(count, outer, *refs), "line",
        (inner_low, rates, *totals, before, token_rows),
        [anywhere()] + [vmem()] * (outer + 3),
        [pltpu.VMEM((heads * held + 2 * heads, HEAD), bf16)] * PLANE + [shape((heads, held // outer, HEAD), bf16)],
        [vmem()] * (PLANE + 1),
        [pltpu.VMEM((outer, heads, held, HEAD), f32), pltpu.VMEM((heads, outer, held, HEAD), f32),
         pltpu.VMEM((heads, outer, held // outer, HEAD), f32), pltpu.VMEM((2 * heads, HEAD), f32)],
        1 << 20)

    arrived = plane_swap(results)
    inner_high, fade_high = inside(heads // 2, "inner_high", results[0])

    mixed, new_read = call(
        lambda *refs: output_kernel(outer, *refs), "output",
        (rates, scaled, inner_low, inner_high, fade_low, fade_high, token_scaled, token_key, token_value,
         norm_gain.reshape(1, width), *arrived),
        [vmem()] * (10 + PLANE),
        [shape((count, width), bf16), shape((1, width), bf16)],
        [hbm(), vmem()],
        [pltpu.VMEM((PLANE, heads * held, HEAD), f32), pltpu.VMEM((PLANE, 2 * heads, HEAD), f32),
         pltpu.VMEM((count, width), bf16), dma((heads // 2,))],
        1 << 20)

    return (mixed.reshape(1, count, width), cache.reshape(1, heads, held // outer, HEAD), new_read)


def shape(dims, dtype):
    return jax.ShapeDtypeStruct(dims, dtype)


def solution(mesh):
    in_specs = (
        P(None, "sp", "tp"),
        P(None, "tp"),
        P(None, "tp"),
        P(None, "tp"),
        P(None, "tp"),
        P("tp"),
        P("tp"),
    )
    out_specs = (P(None, "sp", "tp"), P(None, "tp", "sp", None), P(None, "tp"))
    return jax.shard_map(
        per_device, mesh=mesh, in_specs=in_specs, out_specs=out_specs, check_vma=False
    )
```

```python
import jax
import numpy as np
import jax.numpy as jnp
from jax import lax
from jax.experimental import pallas as pl
from jax.experimental.pallas import tpu as pltpu
from jax.sharding import PartitionSpec as P

HEAD = 128


rope_base = 10000.0
norm_floor = 1e-05


def rotate(tensor, positions):
    head_width = tensor.shape[-1]
    inverse = rope_base ** (-jnp.arange(0, head_width, 2, dtype=jnp.float32) / head_width)
    angles = positions.astype(jnp.float32)[:, None] * inverse[None, :]
    cosine = jnp.cos(angles)[:, None, :]
    sine_part = jnp.sin(angles)[:, None, :]
    first_half = tensor[..., : head_width // 2]
    second_half = tensor[..., head_width // 2 :]
    return jnp.concatenate(
        [
            first_half * cosine - second_half * sine_part,
            first_half * sine_part + second_half * cosine,
        ],
        axis=-1,
    )


def head_norm(output, gain):
    center = jnp.mean(output, axis=-1, keepdims=True)
    spread = jnp.mean(jnp.square(output - center), axis=-1, keepdims=True)
    return (output - center) * lax.rsqrt(spread + norm_floor) * gain


def decay_tables(log_gamma, block_size):
    offsets = jnp.arange(block_size, dtype=jnp.float32)
    gap_table = offsets[:, None] - offsets[None, :]
    within = jnp.where(
        gap_table[None] >= 0,
        jnp.exp(jnp.maximum(gap_table, 0.0)[None] * log_gamma[:, None, None]),
        0.0,
    )
    query_decay = jnp.exp((offsets[:, None] + 1.0) * log_gamma[None, :])
    key_decay = jnp.exp((block_size - 1.0 - offsets[:, None]) * log_gamma[None, :])
    return (within, query_decay, key_decay)


def plain_device(prompt, new_token, w_query, w_key, w_value, decay_rate, norm_gain):
    sequences, block_size, feature_part = prompt.shape
    head_count = w_query.shape[1] // HEAD
    members = lax.axis_size("sp")
    device_rank = lax.axis_index("sp")
    prompt_rows = sequences * block_size
    token_rows = jnp.concatenate([prompt.reshape(prompt_rows, feature_part), new_token], axis=0)
    weight_list = (w_query, w_key, w_value)
    shard_piece = lax.all_gather(token_rows, "tp", axis=1, tiled=True)
    projected = tuple(
        (jnp.dot(shard_piece, weight, preferred_element_type=jnp.float32) for weight in weight_list)
    )
    full_shape = (sequences, block_size, head_count, HEAD)
    queries, key_rows, values = [
        tensor[:prompt_rows].astype(jnp.bfloat16).reshape(full_shape) for tensor in projected
    ]
    token_query, token_key, token_value = [
        tensor[prompt_rows:].astype(jnp.bfloat16).reshape(sequences, 1, head_count, HEAD)
        for tensor in projected
    ]
    positions = device_rank * block_size + jnp.arange(block_size, dtype=jnp.int32)
    scaled = (rotate(queries.astype(jnp.float32), positions) * HEAD ** (-0.5)).astype(jnp.bfloat16)
    turned = rotate(key_rows.astype(jnp.float32), positions).astype(jnp.bfloat16)
    log_gamma = -decay_rate
    within, query_decay, key_decay = decay_tables(log_gamma, block_size)
    weighted = (turned.astype(jnp.float32) * key_decay[None, :, :, None]).astype(jnp.bfloat16)
    local_state = jnp.einsum(
        "smhd,smhe->shde", weighted, values, preferred_element_type=jnp.float32
    )
    pieces = lax.all_to_all(local_state[None], "sp", split_axis=3, concat_axis=0, tiled=True)
    source_index = jnp.arange(members, dtype=jnp.float32)
    gap_table = source_index[:, None] - 1.0 - source_index[None, :]
    weights = jnp.where(
        gap_table[None] >= 0,
        jnp.exp(jnp.maximum(gap_table, 0.0)[None] * block_size * log_gamma[:, None, None]),
        0.0,
    )
    prefix = jnp.einsum("hji,ishre->jshre", weights, pieces, precision=lax.Precision.HIGHEST)
    tail_all = jnp.exp((members - 1.0 - source_index)[None, :] * block_size * log_gamma[:, None])
    final_rows = jnp.einsum("hi,ishre->shre", tail_all, pieces, precision=lax.Precision.HIGHEST)
    incoming = lax.all_to_all(
        prefix.astype(jnp.bfloat16), "sp", split_axis=0, concat_axis=3, tiled=True
    ).astype(prefix.dtype)[0]
    scores = (
        jnp.einsum("snhd,smhd->shnm", scaled, turned, preferred_element_type=jnp.float32)
        * within[None]
    )
    inner_part = jnp.einsum(
        "shnm,smhe->snhe", scores.astype(jnp.bfloat16), values, preferred_element_type=jnp.float32
    )
    carried = (
        jnp.einsum(
            "snhd,shde->snhe",
            scaled,
            incoming.astype(jnp.bfloat16),
            preferred_element_type=jnp.float32,
        )
        * query_decay[None, :, :, None]
    )
    gain = norm_gain.reshape(head_count, HEAD)
    mixed = (
        head_norm(inner_part + carried, gain)
        .astype(jnp.bfloat16)
        .reshape(sequences, block_size, head_count * HEAD)
    )
    cache = final_rows.astype(jnp.bfloat16)
    token_positions = jnp.full((1,), block_size * members, jnp.int32)
    token_scaled = (
        rotate(token_query.astype(jnp.float32), token_positions) * HEAD ** (-0.5)
    ).astype(jnp.bfloat16)[:, 0]
    token_turned = rotate(token_key.astype(jnp.float32), token_positions).astype(jnp.bfloat16)[:, 0]
    row_count = final_rows.shape[2]
    query_rows = lax.dynamic_slice_in_dim(
        token_scaled, device_rank * row_count, row_count, 2
    ).astype(jnp.float32)
    partial_value = jnp.einsum(
        "shr,shre->she", query_rows, final_rows, precision=lax.Precision.HIGHEST
    )
    read_sum = lax.psum(partial_value, "sp")
    own_score = jnp.sum(
        token_scaled.astype(jnp.float32) * token_turned.astype(jnp.float32), axis=-1, keepdims=True
    )
    read_out = jnp.exp(log_gamma)[None, :, None] * read_sum + own_score * token_value[:, 0].astype(
        jnp.float32
    )
    new_read = head_norm(read_out, gain).astype(jnp.bfloat16).reshape(sequences, head_count * HEAD)
    return (mixed, cache, new_read)


PLANE = 4
TOKEN_ROWS = 16
WIDE = 2 * HEAD
BROAD = 4 * HEAD
LOW = 2
f32 = jnp.float32
bf16 = jnp.bfloat16


def vmem():
    return pl.BlockSpec(memory_space=pltpu.VMEM)


def hbm():
    return pl.BlockSpec(memory_space=pltpu.HBM)


def anywhere():
    return pl.BlockSpec(memory_space=pl.ANY)


def far(array):
    return pltpu.with_memory_space_constraint(array, pltpu.HBM)


def params():
    return pltpu.CompilerParams(vmem_limit_bytes=14 * 1024 * 1024)


def cost(flops):
    return pl.CostEstimate(flops=int(flops), transcendentals=0, bytes_accessed=1 << 20)


def place():
    rank = lax.axis_index("sp")
    return rank % PLANE, rank // PLANE


def angle_tables(count, members):
    lane = np.arange(HEAD)
    inverse = rope_base ** (-2.0 * (lane % (HEAD // 2)) / HEAD)
    near = np.arange(count)[:, None] * inverse
    starts = (np.arange(members + 1) * count)[:, None] * inverse
    return [np.float32(f(angles)) for angles in (near, starts) for f in (np.cos, np.sin)]


def own_kernel(own, token_own, w_key, w_value, rate, near_cos, near_sin, starts,
               rows, partial, key_rest, cosine, sine, rates,
               weights, token, angles, bases, scalars, sems):
    count, part = own.shape
    width = w_key.shape[1]
    chunks = width // BROAD
    near = pl.ds(pl.multiple_of(lax.axis_index("tp") * part, part), part)
    rest = pl.ds(pl.multiple_of((1 - lax.axis_index("tp")) * part, part), part)
    copies = []

    def copy(source, target):
        copies.append(pltpu.make_async_copy(source, target, sems.at[len(copies)]))
        copies[-1].start()

    copy(token_own, token)
    copy(own, rows.at[pl.ds(0, count), :])
    for index, matrix in enumerate((w_key, w_value)):
        for chunk in range(chunks):
            columns = pl.ds(chunk * BROAD, BROAD)
            copy(matrix.at[near, columns], weights.at[index, :, columns])
    late = len(copies)
    copy(rate, scalars)
    copy(starts, bases)
    copy(near_cos, angles.at[0])
    copy(near_sin, angles.at[1])
    copy(w_key.at[rest, :], key_rest)
    copies[0].wait()
    copies[1].wait()
    rows[pl.ds(count, TOKEN_ROWS), :] = jnp.broadcast_to(token[...], (TOKEN_ROWS, part))
    for index in range(2):
        for chunk in range(chunks):
            columns = slice(chunk * BROAD, (chunk + 1) * BROAD)
            copies[2 + index * chunks + chunk].wait()
            if index == 1 and chunk == chunks - 1:
                for item in copies[late:-1]:
                    item.wait()
                rank = lax.axis_index("sp")
                last = starts.shape[1] - 1
                sign = jnp.where(lax.broadcasted_iota(jnp.int32, (1, HEAD), 1) < HEAD // 2, -1.0, 1.0)
                base_cos, base_sin = bases[0, pl.ds(rank, 1), :], bases[1, pl.ds(rank, 1), :]
                cosine[pl.ds(0, count), :] = angles[0] * base_cos - angles[1] * base_sin
                sine[pl.ds(0, count), :] = (angles[1] * base_cos + angles[0] * base_sin) * sign
                tail = (TOKEN_ROWS, HEAD)
                cosine[pl.ds(count, TOKEN_ROWS), :] = jnp.broadcast_to(bases[0, last:, :], tail)
                sine[pl.ds(count, TOKEN_ROWS), :] = jnp.broadcast_to(bases[1, last:, :] * sign, tail)
                for head in range(rates.shape[0]):
                    rates[head:head + 1, :] = jnp.full((1, HEAD), scalars[head], f32)
            share = jnp.dot(rows[...], weights[index, :, columns], preferred_element_type=f32)
            for lane in range(BROAD // HEAD):
                partial[(index * width + chunk * BROAD) // HEAD + lane] = share[:, lane * HEAD:(lane + 1) * HEAD]
    copies[-1].wait()


def turn(rows, cosine, sine):
    return rows * cosine + pltpu.roll(rows, HEAD // 2, axis=1) * sine


def into_parts(matrix, parts, outer):
    rest = HEAD // (outer * PLANE)
    split = matrix.reshape(outer, PLANE, rest, HEAD)
    for member in range(PLANE):
        parts[member] = split[:, member].reshape(outer * rest, HEAD)


def key_value_kernel(outer, other, token_other, partial, key_rest, cosine, sine, rates, w_value, w_query,
                     rows, turned, values, token_key, token_value, query_weights, *tail):
    pieces, (value_rest, weighted, parts, sems) = tail[:PLANE], tail[PLANE:]
    member, _ = place()
    count, part = other.shape
    width = key_rest.shape[1]
    own = pl.ds(pl.multiple_of(lax.axis_index("tp") * part, part), part)
    rest = pl.ds(pl.multiple_of((1 - lax.axis_index("tp")) * part, part), part)
    third = pltpu.make_async_copy(w_value.at[rest, :], value_rest, sems.at[2])
    first = pltpu.make_async_copy(w_query.at[own, :], query_weights.at[0], sems.at[0])
    second = pltpu.make_async_copy(w_query.at[rest, :], query_weights.at[1], sems.at[1])
    third.start()
    first.start()
    second.start()
    rows[pl.ds(0, count), :] = other[...]
    rows[pl.ds(count, TOKEN_ROWS), :] = jnp.broadcast_to(token_other[...], (TOKEN_ROWS, part))
    offsets = lax.broadcasted_iota(jnp.int32, (count, HEAD), 0).astype(f32)
    lanes = BROAD // HEAD
    for chunk in range(width // BROAD):
        broad = slice(chunk * BROAD, (chunk + 1) * BROAD)
        key_rows = jnp.dot(rows[...], key_rest[:, broad], preferred_element_type=f32)
        for lane in range(lanes):
            head = chunk * lanes + lane
            inside = slice(lane * HEAD, (lane + 1) * HEAD)
            columns = slice(head * HEAD, (head + 1) * HEAD)
            head_rows = (partial[head] + key_rows[:, inside]).astype(bf16).astype(f32)
            result = turn(head_rows, cosine[...], sine[...]).astype(bf16)
            turned[head] = result[:count]
            token_key[head] = result[count:]
            decay = jnp.exp((offsets - (count - 1.0)) * rates[head:head + 1, :])
            weighted[head] = (result[:count].astype(f32) * decay).astype(bf16)
    third.wait()
    for chunk in range(width // BROAD):
        broad = slice(chunk * BROAD, (chunk + 1) * BROAD)
        value_rows = jnp.dot(rows[...], value_rest[:, broad], preferred_element_type=f32)
        for lane in range(lanes):
            head = chunk * lanes + lane
            inside = slice(lane * HEAD, (lane + 1) * HEAD)
            columns = slice(head * HEAD, (head + 1) * HEAD)
            head_rows = (partial[width // HEAD + head] + value_rows[:, inside]).astype(bf16)
            values[head] = head_rows[:count]
            token_value[head] = head_rows[count:]
            local = lax.dot_general(weighted[head], head_rows[:count], (((0,), (0,)), ((), ())),
                                    preferred_element_type=f32)
            into_parts(local, parts.at[head], outer)
            for r in range(PLANE):
                pieces[r][head] = parts[head, member ^ r].astype(bf16)
    first.wait()
    second.wait()


def query_kernel(outer, chunk, own_rows, other_rows, query_weights, cosine, sine, _, scaled, token_scaled, token_rows, parts):
    member, _ = place()
    heads, count, _ = scaled.shape
    broad = slice(chunk * BROAD, (chunk + 1) * BROAD)
    queries = jnp.dot(own_rows[...], query_weights[0, :, broad], preferred_element_type=f32) + jnp.dot(
        other_rows[...], query_weights[1, :, broad], preferred_element_type=f32)
    queries = queries.astype(bf16).astype(f32)
    for head in range(heads):
        inside = slice(head * HEAD, (head + 1) * HEAD)
        result = (turn(queries[:, inside], cosine[...], sine[...]) * HEAD ** (-0.5)).astype(bf16)
        scaled[head] = result[:count]
        token_scaled[head] = result[count:]
        token = jnp.broadcast_to(result[count:].astype(f32)[:1], (HEAD, HEAD))
        into_parts(token.T, parts.at[head], outer)
        token_rows[head] = parts[head, member]


def chosen(low, high, head):
    return (low, head) if head < low.shape[0] else (high, head - low.shape[0])


def inner_kernel(start, rates, scaled_low, scaled_high, turned, values, _, inner, fade):
    heads, count, _ = inner.shape
    half = count // 2
    lanes = lax.broadcasted_iota(jnp.int32, (1, count), 1).astype(f32)
    offsets = lax.broadcasted_iota(jnp.int32, (count, HEAD), 0).astype(f32)
    keep = lax.broadcasted_iota(jnp.int32, (half, half), 0) >= lax.broadcasted_iota(jnp.int32, (half, half), 1)
    center = centering(HEAD)
    for index in range(heads):
        head = start + index
        scaled, at = chosen(scaled_low, scaled_high, head)
        growth = jnp.exp(lanes * rates[head:head + 1, :1])
        decay = jnp.exp(-offsets * rates[head:head + 1, :])
        fade[index] = decay * jnp.exp(-rates[head:head + 1, :])

        def products(n, m):
            raw = lax.dot_general(scaled[at, n * half:(n + 1) * half], turned[head, m * half:(m + 1) * half],
                                  (((1,), (1,)), ((), ())), preferred_element_type=f32)
            raw = raw * growth[:, m * half:(m + 1) * half]
            return (jnp.where(keep, raw, 0.0) if n == m else raw).astype(bf16)

        centered = jnp.dot(values[head], center, preferred_element_type=f32).astype(bf16)
        low, high = centered[:half], centered[half:]
        inner[index, :half] = jnp.dot(products(0, 0), low, preferred_element_type=f32) * decay[:half]
        inner[index, half:] = (jnp.dot(products(1, 0), low, preferred_element_type=f32) + jnp.dot(
            products(1, 1), high, preferred_element_type=f32)) * decay[half:]


def plane_kernel(count, _, rates, *refs):
    pieces, (total, before, parts) = refs[:PLANE], refs[PLANE:]
    member, _ = place()
    for r in range(PLANE):
        parts[member ^ r] = pieces[r][...].astype(f32)
    for head in range(total.shape[0]):
        factor = jnp.exp(rates[head:head + 1, :] * -count)
        state = jnp.zeros(total.shape[1:], f32)
        for source in range(PLANE):
            before[source, head] = state
            state = state * factor + parts[source, head]
        total[head] = state.astype(bf16)


def line_kernel(count, outer, _, rates, *refs):
    totals = refs[:outer]
    before, token_rows_low, token_rows_high = refs[outer:outer + 3]
    results, cache = refs[outer + 3:outer + 3 + PLANE], refs[outer + 3 + PLANE]
    ordered, running, final, reads = refs[outer + 4 + PLANE:]
    member, line = place()
    heads, width = totals[0].shape[:2]
    for s in range(outer):
        ordered[line ^ s] = totals[s][...].astype(f32)
    for head in range(heads):
        log_factor = rates[head:head + 1, :] * -count
        factor = jnp.exp(log_factor * PLANE)
        state = jnp.zeros((width, HEAD), f32)
        for source in range(outer):
            running[head, source] = state
            state = state * factor + ordered[source, head]
        final[head] = state.reshape(final.shape[1:])
        cache[head] = final[head, line].astype(bf16)
        token_rows, at = chosen(token_rows_low, token_rows_high, head)
        read = jnp.sum(token_rows[at] * state, axis=0, keepdims=True)
        high = read.astype(bf16).astype(f32)
        reads[head:head + 1, :] = high
        reads[heads + head:heads + head + 1, :] = read - high
        arriving = running[head, line]
        for r in range(PLANE):
            scale = jnp.exp(log_factor * (member ^ r).astype(f32))
            results[r][pl.ds(head * width, width), :] = (before[member ^ r, head] + scale * arriving).astype(bf16)
    for r in range(PLANE):
        results[r][pl.ds(heads * width, 2 * heads), :] = reads[...].astype(bf16)


def centering(size):
    rows_of = lax.broadcasted_iota(jnp.int32, (size, size), 0)
    columns_of = lax.broadcasted_iota(jnp.int32, (size, size), 1)
    same = jnp.where(rows_of == columns_of, 1.0, 0.0)
    return (same - jnp.where(rows_of // HEAD == columns_of // HEAD, 1.0 / HEAD, 0.0)).astype(bf16)


def finish(rows, gain):
    center = jnp.mean(rows, axis=-1, keepdims=True)
    rows = rows - center
    spread = jnp.mean(jnp.square(rows), axis=-1, keepdims=True)
    return rows * lax.rsqrt(spread + norm_floor) * gain


def output_kernel(outer, rates, scaled_low, scaled_high, inner_low, inner_high, fade_low, fade_high,
                  token_scaled_low, token_scaled_high, token_key, token_value, final, gain, *refs):
    pieces, (mixed, new_read, cache, parts, reads, read_buffer, buffer, sems) = refs[:PLANE], refs[PLANE:]
    member, _ = place()
    heads, count, _ = token_key.shape[0], scaled_low.shape[1], 0
    held = HEAD // PLANE
    copies = [pltpu.make_async_copy(final, cache, sems.at[0])]
    copies[0].start()
    for r in range(PLANE):
        parts[member ^ r] = pieces[r][pl.ds(0, heads * held), :].astype(f32)
        reads[member ^ r] = pieces[r][pl.ds(heads * held, 2 * heads), :].astype(f32)
    sums = reads[0]
    for source in range(1, PLANE):
        sums = sums + reads[source]
    sums = sums[:heads] + sums[heads:]
    for head in range(heads):
        columns = slice(head * HEAD, (head + 1) * HEAD)
        token_scaled, at = chosen(token_scaled_low, token_scaled_high, head)
        query = token_scaled[at].astype(f32)[:1]
        key = token_key[head].astype(f32)[:1]
        value = token_value[head].astype(f32)[:1]
        own_score = jnp.sum(query * key, axis=-1, keepdims=True)
        read = jnp.exp(-rates[head:head + 1, :]) * sums[head:head + 1] + own_score * value
        read_buffer[:, columns] = finish(read, gain[:, columns]).astype(bf16)
    copies.append(pltpu.make_async_copy(read_buffer, new_read, sems.at[1]))
    copies[1].start()
    rows_of = lax.broadcasted_iota(jnp.int32, (WIDE, WIDE), 0) // HEAD
    columns_of = lax.broadcasted_iota(jnp.int32, (WIDE, WIDE), 1) // HEAD
    average = jnp.where(rows_of == columns_of, 1.0 / HEAD, 0.0).astype(bf16)
    center = centering(HEAD)
    blank = jnp.zeros((HEAD, HEAD), bf16)

    def both(low, high, head):
        sides = [chosen(low, high, head), chosen(low, high, head + 1)]
        return jnp.concatenate([side[at] for side, at in sides], axis=1)

    for pair in range(heads // 2):
        wide = slice(pair * WIDE, (pair + 1) * WIDE)
        states = []
        for head in (2 * pair, 2 * pair + 1):
            split = [parts[source, pl.ds(head * held, held), :].reshape(outer, 1, held // outer, HEAD) for source in range(PLANE)]
            state = jnp.concatenate(split, axis=1).reshape(HEAD, HEAD).astype(bf16)
            states.append(jnp.dot(state, center, preferred_element_type=f32).astype(bf16))
        incoming = jnp.concatenate([jnp.concatenate([states[0], blank], axis=1), jnp.concatenate([blank, states[1]], axis=1)], axis=0)
        carried = jnp.dot(both(scaled_low, scaled_high, 2 * pair), incoming, preferred_element_type=f32)
        rows = both(inner_low, inner_high, 2 * pair) + carried * both(fade_low, fade_high, 2 * pair)
        spread = jnp.dot((rows * rows).astype(bf16), average, preferred_element_type=f32)
        buffer[pair] = (rows * lax.rsqrt(spread + norm_floor) * gain[:, wide]).astype(bf16)
        copies.append(pltpu.make_async_copy(buffer.at[pair], mixed.at[:, pl.ds(pair * WIDE, WIDE)], sems.at[2 + pair]))
        copies[-1].start()
    for copy in copies:
        copy.wait()


def per_device(prompt, new_token, w_query, w_key, w_value, decay_rate, norm_gain):
    members = lax.axis_size("sp")
    heads = w_query.shape[1] // HEAD
    sequences, count, part = prompt.shape
    if (lax.axis_size("tp") != 2 or members % PLANE or HEAD % (8 * members) or sequences != 1 or heads * HEAD != 2 * BROAD
            or count % 256 or count > 1024):
        return plain_device(prompt, new_token, w_query, w_key, w_value, decay_rate, norm_gain)
    outer = members // PLANE
    held = HEAD // PLANE
    width = heads * HEAD
    total_rows = count + TOKEN_ROWS
    own = prompt.reshape(count, part)
    swap = [(0, 1), (1, 0)]
    other = lax.ppermute(own, "tp", swap)
    token_other = lax.ppermute(new_token, "tp", swap)
    dma = pltpu.SemaphoreType.DMA

    def call(kernel, name, arguments, specs, outs, out_specs, scratch, flops):
        return pl.pallas_call(kernel, in_specs=specs, out_specs=out_specs, out_shape=outs, scratch_shapes=scratch,
                              compiler_params=params(), cost_estimate=cost(flops), name=name)(*arguments)

    near_cos, near_sin, start_cos, start_sin = angle_tables(count, members)
    near_cos, near_sin, starts = jnp.asarray(near_cos), jnp.asarray(near_sin), jnp.asarray(np.stack([start_cos, start_sin]))
    rows, partial, key_rest, cosine, sine, rates = call(
        own_kernel, "own",
        (far(own), far(new_token), far(w_key), far(w_value), far(decay_rate), far(near_cos), far(near_sin), far(starts)),
        [hbm()] * 8,
        [pltpu.VMEM((total_rows, part), bf16), pltpu.VMEM((2 * heads, total_rows, HEAD), f32), pltpu.VMEM((part, width), bf16),
         pltpu.VMEM((total_rows, HEAD), f32), pltpu.VMEM((total_rows, HEAD), f32), pltpu.VMEM((heads, HEAD), f32)],
        [vmem()] * 6,
        [pltpu.VMEM((2, part, width), bf16), pltpu.VMEM((1, part), bf16), pltpu.VMEM((2, count, HEAD), f32),
         pltpu.VMEM(starts.shape, f32), pltpu.SMEM((heads,), f32), dma((7 + 2 * width // BROAD,))],
        4 * total_rows * part * width)

    other_rows, turned, values, token_key, token_value, query_weights, *pieces = call(
        lambda *refs: key_value_kernel(outer, *refs), "key_value",
        (other, token_other, partial, key_rest, cosine, sine, rates, far(w_value), far(w_query)),
        [vmem()] * 7 + [hbm()] * 2,
        [pltpu.VMEM((total_rows, part), bf16), pltpu.VMEM((heads, count, HEAD), bf16), pltpu.VMEM((heads, count, HEAD), bf16),
         pltpu.VMEM((heads, TOKEN_ROWS, HEAD), bf16), pltpu.VMEM((heads, TOKEN_ROWS, HEAD), bf16), pltpu.VMEM((2, part, width), bf16)]
        + [pltpu.VMEM((heads, held, HEAD), bf16)] * PLANE,
        [vmem()] * (6 + PLANE),
        [pltpu.VMEM((part, width), bf16), pltpu.VMEM((heads, count, HEAD), bf16), pltpu.VMEM((heads, PLANE, held, HEAD), f32), dma((3,))],
        4 * total_rows * part * width)

    def plane_swap(items):
        return [items[0]] + [
            lax.ppermute(items[r], "sp", [(s, s ^ r) for s in range(members)]) for r in range(1, PLANE)
        ]

    gathered = plane_swap(pieces)

    def query(chunk, name, after):
        span = BROAD // HEAD
        return call(
            lambda *refs: query_kernel(outer, chunk, *refs), name,
            (rows, other_rows, query_weights, cosine, sine, after),
            [vmem()] * 5 + [anywhere()],
            [pltpu.VMEM((span, count, HEAD), bf16), pltpu.VMEM((span, TOKEN_ROWS, HEAD), bf16), pltpu.VMEM((span, held, HEAD), f32)],
            [vmem()] * 3,
            [pltpu.VMEM((span, PLANE, held, HEAD), f32)],
            4 * total_rows * part * BROAD)

    scaled_low, token_scaled_low, token_rows_low = query(0, "query_low", rates)

    total, before = call(
        lambda *refs: plane_kernel(count, *refs), "plane",
        (token_scaled_low, rates, *gathered),
        [anywhere()] + [vmem()] * (1 + PLANE),
        [pltpu.VMEM((heads, held, HEAD), bf16), pltpu.VMEM((PLANE, heads, held, HEAD), f32)],
        [vmem()] * 2,
        [pltpu.VMEM((PLANE, heads, held, HEAD), f32)],
        1 << 20)

    totals = [total] + [
        lax.ppermute(total, "sp", [(s, s ^ (PLANE * r)) for s in range(members)]) for r in range(1, outer)
    ]

    scaled_high, token_scaled_high, token_rows_high = query(1, "query_high", total)

    def inside(start, units, name, after):
        return call(
            lambda *refs: inner_kernel(start, *refs), name,
            (rates, scaled_low, scaled_high, turned, values, after),
            [vmem()] * 5 + [anywhere()], [pltpu.VMEM((units, count, HEAD), f32)] * 2, [vmem()] * 2, [],
            4 * count * count * units * HEAD)

    inner_low, fade_low = inside(0, LOW, "inner_low", total)

    *results, final = call(
        lambda *refs: line_kernel(count, outer, *refs), "line",
        (inner_low, rates, *totals, before, token_rows_low, token_rows_high),
        [anywhere()] + [vmem()] * (outer + 4),
        [pltpu.VMEM((heads * held + 2 * heads, HEAD), bf16)] * PLANE + [pltpu.VMEM((heads, held // outer, HEAD), bf16)],
        [vmem()] * (PLANE + 1),
        [pltpu.VMEM((outer, heads, held, HEAD), f32), pltpu.VMEM((heads, outer, held, HEAD), f32),
         pltpu.VMEM((heads, outer, held // outer, HEAD), f32), pltpu.VMEM((2 * heads, HEAD), f32)],
        1 << 20)

    arrived = plane_swap(results)
    inner_high, fade_high = inside(LOW, heads - LOW, "inner_high", results[0])

    mixed, new_read, cache = call(
        lambda *refs: output_kernel(outer, *refs), "output",
        (rates, scaled_low, scaled_high, inner_low, inner_high, fade_low, fade_high, token_scaled_low, token_scaled_high,
         token_key, token_value, final, norm_gain.reshape(1, width), *arrived),
        [vmem()] * (13 + PLANE),
        [shape((count, width), bf16), shape((1, width), bf16), shape((heads, held // outer, HEAD), bf16)],
        [hbm()] * 3,
        [pltpu.VMEM((PLANE, heads * held, HEAD), f32), pltpu.VMEM((PLANE, 2 * heads, HEAD), f32), pltpu.VMEM((1, width), bf16),
         pltpu.VMEM((heads // 2, count, WIDE), bf16), dma((2 + heads // 2,))],
        1 << 20)

    return (mixed.reshape(1, count, width), cache.reshape(1, heads, held // outer, HEAD), new_read)


def shape(dims, dtype):
    return jax.ShapeDtypeStruct(dims, dtype)


def solution(mesh):
    in_specs = (
        P(None, "sp", "tp"),
        P(None, "tp"),
        P(None, "tp"),
        P(None, "tp"),
        P(None, "tp"),
        P("tp"),
        P("tp"),
    )
    out_specs = (P(None, "sp", "tp"), P(None, "tp", "sp", None), P(None, "tp"))
    return jax.shard_map(
        per_device, mesh=mesh, in_specs=in_specs, out_specs=out_specs, check_vma=False
    )
```

```python
import jax
import numpy as np
import jax.numpy as jnp
from jax import lax
from jax.experimental import pallas as pl
from jax.experimental.pallas import tpu as pltpu
from jax.sharding import PartitionSpec as P

HEAD = 128


rope_base = 10000.0
norm_floor = 1e-05


def rotate(tensor, positions):
    head_width = tensor.shape[-1]
    inverse = rope_base ** (-jnp.arange(0, head_width, 2, dtype=jnp.float32) / head_width)
    angles = positions.astype(jnp.float32)[:, None] * inverse[None, :]
    cosine = jnp.cos(angles)[:, None, :]
    sine_part = jnp.sin(angles)[:, None, :]
    first_half = tensor[..., : head_width // 2]
    second_half = tensor[..., head_width // 2 :]
    return jnp.concatenate(
        [
            first_half * cosine - second_half * sine_part,
            first_half * sine_part + second_half * cosine,
        ],
        axis=-1,
    )


def head_norm(output, gain):
    center = jnp.mean(output, axis=-1, keepdims=True)
    spread = jnp.mean(jnp.square(output - center), axis=-1, keepdims=True)
    return (output - center) * lax.rsqrt(spread + norm_floor) * gain


def decay_tables(log_gamma, block_size):
    offsets = jnp.arange(block_size, dtype=jnp.float32)
    gap_table = offsets[:, None] - offsets[None, :]
    within = jnp.where(
        gap_table[None] >= 0,
        jnp.exp(jnp.maximum(gap_table, 0.0)[None] * log_gamma[:, None, None]),
        0.0,
    )
    query_decay = jnp.exp((offsets[:, None] + 1.0) * log_gamma[None, :])
    key_decay = jnp.exp((block_size - 1.0 - offsets[:, None]) * log_gamma[None, :])
    return (within, query_decay, key_decay)


def plain_device(prompt, new_token, w_query, w_key, w_value, decay_rate, norm_gain):
    sequences, block_size, feature_part = prompt.shape
    head_count = w_query.shape[1] // HEAD
    members = lax.axis_size("sp")
    device_rank = lax.axis_index("sp")
    prompt_rows = sequences * block_size
    token_rows = jnp.concatenate([prompt.reshape(prompt_rows, feature_part), new_token], axis=0)
    weight_list = (w_query, w_key, w_value)
    shard_piece = lax.all_gather(token_rows, "tp", axis=1, tiled=True)
    projected = tuple(
        (jnp.dot(shard_piece, weight, preferred_element_type=jnp.float32) for weight in weight_list)
    )
    full_shape = (sequences, block_size, head_count, HEAD)
    queries, key_rows, values = [
        tensor[:prompt_rows].astype(jnp.bfloat16).reshape(full_shape) for tensor in projected
    ]
    token_query, token_key, token_value = [
        tensor[prompt_rows:].astype(jnp.bfloat16).reshape(sequences, 1, head_count, HEAD)
        for tensor in projected
    ]
    positions = device_rank * block_size + jnp.arange(block_size, dtype=jnp.int32)
    scaled = (rotate(queries.astype(jnp.float32), positions) * HEAD ** (-0.5)).astype(jnp.bfloat16)
    turned = rotate(key_rows.astype(jnp.float32), positions).astype(jnp.bfloat16)
    log_gamma = -decay_rate
    within, query_decay, key_decay = decay_tables(log_gamma, block_size)
    weighted = (turned.astype(jnp.float32) * key_decay[None, :, :, None]).astype(jnp.bfloat16)
    local_state = jnp.einsum(
        "smhd,smhe->shde", weighted, values, preferred_element_type=jnp.float32
    )
    pieces = lax.all_to_all(local_state[None], "sp", split_axis=3, concat_axis=0, tiled=True)
    source_index = jnp.arange(members, dtype=jnp.float32)
    gap_table = source_index[:, None] - 1.0 - source_index[None, :]
    weights = jnp.where(
        gap_table[None] >= 0,
        jnp.exp(jnp.maximum(gap_table, 0.0)[None] * block_size * log_gamma[:, None, None]),
        0.0,
    )
    prefix = jnp.einsum("hji,ishre->jshre", weights, pieces, precision=lax.Precision.HIGHEST)
    tail_all = jnp.exp((members - 1.0 - source_index)[None, :] * block_size * log_gamma[:, None])
    final_rows = jnp.einsum("hi,ishre->shre", tail_all, pieces, precision=lax.Precision.HIGHEST)
    incoming = lax.all_to_all(
        prefix.astype(jnp.bfloat16), "sp", split_axis=0, concat_axis=3, tiled=True
    ).astype(prefix.dtype)[0]
    scores = (
        jnp.einsum("snhd,smhd->shnm", scaled, turned, preferred_element_type=jnp.float32)
        * within[None]
    )
    inner_part = jnp.einsum(
        "shnm,smhe->snhe", scores.astype(jnp.bfloat16), values, preferred_element_type=jnp.float32
    )
    carried = (
        jnp.einsum(
            "snhd,shde->snhe",
            scaled,
            incoming.astype(jnp.bfloat16),
            preferred_element_type=jnp.float32,
        )
        * query_decay[None, :, :, None]
    )
    gain = norm_gain.reshape(head_count, HEAD)
    mixed = (
        head_norm(inner_part + carried, gain)
        .astype(jnp.bfloat16)
        .reshape(sequences, block_size, head_count * HEAD)
    )
    cache = final_rows.astype(jnp.bfloat16)
    token_positions = jnp.full((1,), block_size * members, jnp.int32)
    token_scaled = (
        rotate(token_query.astype(jnp.float32), token_positions) * HEAD ** (-0.5)
    ).astype(jnp.bfloat16)[:, 0]
    token_turned = rotate(token_key.astype(jnp.float32), token_positions).astype(jnp.bfloat16)[:, 0]
    row_count = final_rows.shape[2]
    query_rows = lax.dynamic_slice_in_dim(
        token_scaled, device_rank * row_count, row_count, 2
    ).astype(jnp.float32)
    partial_value = jnp.einsum(
        "shr,shre->she", query_rows, final_rows, precision=lax.Precision.HIGHEST
    )
    read_sum = lax.psum(partial_value, "sp")
    own_score = jnp.sum(
        token_scaled.astype(jnp.float32) * token_turned.astype(jnp.float32), axis=-1, keepdims=True
    )
    read_out = jnp.exp(log_gamma)[None, :, None] * read_sum + own_score * token_value[:, 0].astype(
        jnp.float32
    )
    new_read = head_norm(read_out, gain).astype(jnp.bfloat16).reshape(sequences, head_count * HEAD)
    return (mixed, cache, new_read)


PLANE = 4
TOKEN_ROWS = 16
WIDE = 2 * HEAD
BROAD = 4 * HEAD
LOW = 2
f32 = jnp.float32
bf16 = jnp.bfloat16


def vmem():
    return pl.BlockSpec(memory_space=pltpu.VMEM)


def hbm():
    return pl.BlockSpec(memory_space=pltpu.HBM)


def anywhere():
    return pl.BlockSpec(memory_space=pl.ANY)


def far(array):
    return pltpu.with_memory_space_constraint(array, pltpu.HBM)


def params():
    return pltpu.CompilerParams(vmem_limit_bytes=14 * 1024 * 1024)


def cost(flops):
    return pl.CostEstimate(flops=int(flops), transcendentals=0, bytes_accessed=1 << 20)


def place():
    rank = lax.axis_index("sp")
    return rank % PLANE, rank // PLANE


def angle_tables(count, members):
    lane = np.arange(HEAD)
    inverse = rope_base ** (-2.0 * (lane % (HEAD // 2)) / HEAD)
    near = np.arange(count)[:, None] * inverse
    starts = (np.arange(members + 1) * count)[:, None] * inverse
    return [np.float32(f(angles)) for angles in (near, starts) for f in (np.cos, np.sin)]


def own_kernel(own, token_own, w_key, w_value, rate, near_cos, near_sin, starts,
               rows, partial, key_rest, value_rest, cosine, sine, rates,
               weights, token, angles, bases, scalars, sems):
    count, part = own.shape
    width = w_key.shape[1]
    chunks = width // BROAD
    near = pl.ds(pl.multiple_of(lax.axis_index("tp") * part, part), part)
    rest = pl.ds(pl.multiple_of((1 - lax.axis_index("tp")) * part, part), part)
    copies = []

    def copy(source, target):
        copies.append(pltpu.make_async_copy(source, target, sems.at[len(copies)]))
        copies[-1].start()

    copy(token_own, token)
    copy(own, rows.at[pl.ds(0, count), :])
    for index, matrix in enumerate((w_key, w_value)):
        for chunk in range(chunks):
            columns = pl.ds(chunk * BROAD, BROAD)
            copy(matrix.at[near, columns], weights.at[index, :, columns])
    late = len(copies)
    copy(rate, scalars)
    copy(starts, bases)
    copy(near_cos, angles.at[0])
    copy(near_sin, angles.at[1])
    last_tables = len(copies)
    copy(w_key.at[rest, :], key_rest)
    copy(w_value.at[rest, :], value_rest)
    copies[0].wait()
    copies[1].wait()
    rows[pl.ds(count, TOKEN_ROWS), :] = jnp.broadcast_to(token[...], (TOKEN_ROWS, part))
    for index in range(2):
        for chunk in range(chunks):
            columns = slice(chunk * BROAD, (chunk + 1) * BROAD)
            copies[2 + index * chunks + chunk].wait()
            if index == 1 and chunk == chunks - 1:
                for item in copies[late:last_tables]:
                    item.wait()
                rank = lax.axis_index("sp")
                last = starts.shape[1] - 1
                sign = jnp.where(lax.broadcasted_iota(jnp.int32, (1, HEAD), 1) < HEAD // 2, -1.0, 1.0)
                base_cos, base_sin = bases[0, pl.ds(rank, 1), :], bases[1, pl.ds(rank, 1), :]
                cosine[pl.ds(0, count), :] = angles[0] * base_cos - angles[1] * base_sin
                sine[pl.ds(0, count), :] = (angles[1] * base_cos + angles[0] * base_sin) * sign
                tail = (TOKEN_ROWS, HEAD)
                cosine[pl.ds(count, TOKEN_ROWS), :] = jnp.broadcast_to(bases[0, last:, :], tail)
                sine[pl.ds(count, TOKEN_ROWS), :] = jnp.broadcast_to(bases[1, last:, :] * sign, tail)
                for head in range(rates.shape[0]):
                    rates[head:head + 1, :] = jnp.full((1, HEAD), scalars[head], f32)
            share = jnp.dot(rows[...], weights[index, :, columns], preferred_element_type=f32)
            for lane in range(BROAD // HEAD):
                partial[(index * width + chunk * BROAD) // HEAD + lane] = share[:, lane * HEAD:(lane + 1) * HEAD]
    for item in copies[last_tables:]:
        item.wait()


def turn(rows, cosine, sine):
    return rows * cosine + pltpu.roll(rows, HEAD // 2, axis=1) * sine


def into_parts(matrix, parts, outer):
    rest = HEAD // (outer * PLANE)
    split = matrix.reshape(outer, PLANE, rest, HEAD)
    for member in range(PLANE):
        parts[member] = split[:, member].reshape(outer * rest, HEAD)


def key_value_kernel(outer, other, token_other, partial, key_rest, value_rest, cosine, sine, rates,
                     rows, turned, values, token_key, token_value, *tail):
    pieces, (weighted, parts) = tail[:PLANE], tail[PLANE:]
    member, _ = place()
    count, part = other.shape
    width = key_rest.shape[1]
    rows[pl.ds(0, count), :] = other[...]
    rows[pl.ds(count, TOKEN_ROWS), :] = jnp.broadcast_to(token_other[...], (TOKEN_ROWS, part))
    offsets = lax.broadcasted_iota(jnp.int32, (count, HEAD), 0).astype(f32)
    lanes = BROAD // HEAD
    for chunk in range(width // BROAD):
        broad = slice(chunk * BROAD, (chunk + 1) * BROAD)
        key_rows = jnp.dot(rows[...], key_rest[:, broad], preferred_element_type=f32)
        for lane in range(lanes):
            head = chunk * lanes + lane
            inside = slice(lane * HEAD, (lane + 1) * HEAD)
            columns = slice(head * HEAD, (head + 1) * HEAD)
            head_rows = (partial[head] + key_rows[:, inside]).astype(bf16).astype(f32)
            result = turn(head_rows, cosine[...], sine[...]).astype(bf16)
            turned[head] = result[:count]
            token_key[head] = result[count:]
            decay = jnp.exp((offsets - (count - 1.0)) * rates[head:head + 1, :])
            weighted[head] = (result[:count].astype(f32) * decay).astype(bf16)
    for chunk in range(width // BROAD):
        broad = slice(chunk * BROAD, (chunk + 1) * BROAD)
        value_rows = jnp.dot(rows[...], value_rest[:, broad], preferred_element_type=f32)
        for lane in range(lanes):
            head = chunk * lanes + lane
            inside = slice(lane * HEAD, (lane + 1) * HEAD)
            columns = slice(head * HEAD, (head + 1) * HEAD)
            head_rows = (partial[width // HEAD + head] + value_rows[:, inside]).astype(bf16)
            values[head] = head_rows[:count]
            token_value[head] = head_rows[count:]
            local = lax.dot_general(weighted[head], head_rows[:count], (((0,), (0,)), ((), ())),
                                    preferred_element_type=f32)
            into_parts(local, parts.at[head], outer)
            for r in range(PLANE):
                pieces[r][head] = parts[head, member ^ r].astype(bf16)


def query_kernel(outer, chunk, own_rows, other_rows, query_weights, cosine, sine, _, scaled, token_scaled, token_rows, parts):
    member, _ = place()
    heads, count, _ = scaled.shape
    side = lax.axis_index("tp")
    broad = slice(chunk * BROAD, (chunk + 1) * BROAD)
    queries = jnp.dot(own_rows[...], query_weights[side, :, broad], preferred_element_type=f32) + jnp.dot(
        other_rows[...], query_weights[1 - side, :, broad], preferred_element_type=f32)
    queries = queries.astype(bf16).astype(f32)
    for head in range(heads):
        inside = slice(head * HEAD, (head + 1) * HEAD)
        result = (turn(queries[:, inside], cosine[...], sine[...]) * HEAD ** (-0.5)).astype(bf16)
        scaled[head] = result[:count]
        token_scaled[head] = result[count:]
        token = jnp.broadcast_to(result[count:].astype(f32)[:1], (HEAD, HEAD))
        into_parts(token.T, parts.at[head], outer)
        token_rows[head] = parts[head, member]


def chosen(low, high, head):
    return (low, head) if head < low.shape[0] else (high, head - low.shape[0])


def inner_kernel(start, rates, scaled_low, scaled_high, turned, values, _, inner, fade):
    heads, count, _ = inner.shape
    half = count // 2
    lanes = lax.broadcasted_iota(jnp.int32, (1, count), 1).astype(f32)
    offsets = lax.broadcasted_iota(jnp.int32, (count, HEAD), 0).astype(f32)
    keep = lax.broadcasted_iota(jnp.int32, (half, half), 0) >= lax.broadcasted_iota(jnp.int32, (half, half), 1)
    center = centering(HEAD)
    for index in range(heads):
        head = start + index
        scaled, at = chosen(scaled_low, scaled_high, head)
        growth = jnp.exp(lanes * rates[head:head + 1, :1])
        decay = jnp.exp(-offsets * rates[head:head + 1, :])
        fade[index] = decay * jnp.exp(-rates[head:head + 1, :])

        def products(n, m):
            raw = lax.dot_general(scaled[at, n * half:(n + 1) * half], turned[head, m * half:(m + 1) * half],
                                  (((1,), (1,)), ((), ())), preferred_element_type=f32)
            raw = raw * growth[:, m * half:(m + 1) * half]
            return (jnp.where(keep, raw, 0.0) if n == m else raw).astype(bf16)

        centered = jnp.dot(values[head], center, preferred_element_type=f32).astype(bf16)
        low, high = centered[:half], centered[half:]
        inner[index, :half] = jnp.dot(products(0, 0), low, preferred_element_type=f32) * decay[:half]
        inner[index, half:] = (jnp.dot(products(1, 0), low, preferred_element_type=f32) + jnp.dot(
            products(1, 1), high, preferred_element_type=f32)) * decay[half:]


def plane_kernel(count, _, rates, *refs):
    pieces, (total, before, parts) = refs[:PLANE], refs[PLANE:]
    member, _ = place()
    for r in range(PLANE):
        parts[member ^ r] = pieces[r][...].astype(f32)
    for head in range(total.shape[0]):
        factor = jnp.exp(rates[head:head + 1, :] * -count)
        state = jnp.zeros(total.shape[1:], f32)
        for source in range(PLANE):
            before[source, head] = state
            state = state * factor + parts[source, head]
        total[head] = state.astype(bf16)


def line_kernel(count, outer, _, rates, *refs):
    totals = refs[:outer]
    before, token_rows_low, token_rows_high = refs[outer:outer + 3]
    results, cache = refs[outer + 3:outer + 3 + PLANE], refs[outer + 3 + PLANE]
    ordered, running, final, reads = refs[outer + 4 + PLANE:]
    member, line = place()
    heads, width = totals[0].shape[:2]
    for s in range(outer):
        ordered[line ^ s] = totals[s][...].astype(f32)
    for head in range(heads):
        log_factor = rates[head:head + 1, :] * -count
        factor = jnp.exp(log_factor * PLANE)
        state = jnp.zeros((width, HEAD), f32)
        for source in range(outer):
            running[head, source] = state
            state = state * factor + ordered[source, head]
        final[head] = state.reshape(final.shape[1:])
        cache[head] = final[head, line].astype(bf16)
        token_rows, at = chosen(token_rows_low, token_rows_high, head)
        read = jnp.sum(token_rows[at] * state, axis=0, keepdims=True)
        high = read.astype(bf16).astype(f32)
        reads[head:head + 1, :] = high
        reads[heads + head:heads + head + 1, :] = read - high
        arriving = running[head, line]
        for r in range(PLANE):
            scale = jnp.exp(log_factor * (member ^ r).astype(f32))
            results[r][pl.ds(head * width, width), :] = (before[member ^ r, head] + scale * arriving).astype(bf16)
    for r in range(PLANE):
        results[r][pl.ds(heads * width, 2 * heads), :] = reads[...].astype(bf16)


def centering(size):
    rows_of = lax.broadcasted_iota(jnp.int32, (size, size), 0)
    columns_of = lax.broadcasted_iota(jnp.int32, (size, size), 1)
    same = jnp.where(rows_of == columns_of, 1.0, 0.0)
    return (same - jnp.where(rows_of // HEAD == columns_of // HEAD, 1.0 / HEAD, 0.0)).astype(bf16)


def finish(rows, gain):
    center = jnp.mean(rows, axis=-1, keepdims=True)
    rows = rows - center
    spread = jnp.mean(jnp.square(rows), axis=-1, keepdims=True)
    return rows * lax.rsqrt(spread + norm_floor) * gain


def output_kernel(outer, rates, scaled_low, scaled_high, inner_low, inner_high, fade_low, fade_high,
                  token_scaled_low, token_scaled_high, token_key, token_value, final, gain, *refs):
    pieces, (mixed, new_read, cache, parts, reads, read_buffer, buffer, sems) = refs[:PLANE], refs[PLANE:]
    member, _ = place()
    heads, count, _ = token_key.shape[0], scaled_low.shape[1], 0
    held = HEAD // PLANE
    copies = [pltpu.make_async_copy(final, cache, sems.at[0])]
    copies[0].start()
    for r in range(PLANE):
        parts[member ^ r] = pieces[r][pl.ds(0, heads * held), :].astype(f32)
        reads[member ^ r] = pieces[r][pl.ds(heads * held, 2 * heads), :].astype(f32)
    sums = reads[0]
    for source in range(1, PLANE):
        sums = sums + reads[source]
    sums = sums[:heads] + sums[heads:]
    for head in range(heads):
        columns = slice(head * HEAD, (head + 1) * HEAD)
        token_scaled, at = chosen(token_scaled_low, token_scaled_high, head)
        query = token_scaled[at].astype(f32)[:1]
        key = token_key[head].astype(f32)[:1]
        value = token_value[head].astype(f32)[:1]
        own_score = jnp.sum(query * key, axis=-1, keepdims=True)
        read = jnp.exp(-rates[head:head + 1, :]) * sums[head:head + 1] + own_score * value
        read_buffer[:, columns] = finish(read, gain[:, columns]).astype(bf16)
    copies.append(pltpu.make_async_copy(read_buffer, new_read, sems.at[1]))
    copies[1].start()
    rows_of = lax.broadcasted_iota(jnp.int32, (WIDE, WIDE), 0) // HEAD
    columns_of = lax.broadcasted_iota(jnp.int32, (WIDE, WIDE), 1) // HEAD
    average = jnp.where(rows_of == columns_of, 1.0 / HEAD, 0.0).astype(bf16)
    center = centering(HEAD)
    blank = jnp.zeros((HEAD, HEAD), bf16)

    def both(low, high, head):
        sides = [chosen(low, high, head), chosen(low, high, head + 1)]
        return jnp.concatenate([side[at] for side, at in sides], axis=1)

    for pair in range(heads // 2):
        wide = slice(pair * WIDE, (pair + 1) * WIDE)
        states = []
        for head in (2 * pair, 2 * pair + 1):
            split = [parts[source, pl.ds(head * held, held), :].reshape(outer, 1, held // outer, HEAD) for source in range(PLANE)]
            state = jnp.concatenate(split, axis=1).reshape(HEAD, HEAD).astype(bf16)
            states.append(jnp.dot(state, center, preferred_element_type=f32).astype(bf16))
        incoming = jnp.concatenate([jnp.concatenate([states[0], blank], axis=1), jnp.concatenate([blank, states[1]], axis=1)], axis=0)
        carried = jnp.dot(both(scaled_low, scaled_high, 2 * pair), incoming, preferred_element_type=f32)
        rows = both(inner_low, inner_high, 2 * pair) + carried * both(fade_low, fade_high, 2 * pair)
        spread = jnp.dot((rows * rows).astype(bf16), average, preferred_element_type=f32)
        buffer[pair] = (rows * lax.rsqrt(spread + norm_floor) * gain[:, wide]).astype(bf16)
        copies.append(pltpu.make_async_copy(buffer.at[pair], mixed.at[:, pl.ds(pair * WIDE, WIDE)], sems.at[2 + pair]))
        copies[-1].start()
    for copy in copies:
        copy.wait()


def per_device(prompt, new_token, w_query, w_key, w_value, decay_rate, norm_gain):
    members = lax.axis_size("sp")
    heads = w_query.shape[1] // HEAD
    sequences, count, part = prompt.shape
    if (lax.axis_size("tp") != 2 or members % PLANE or HEAD % (8 * members) or sequences != 1 or heads * HEAD != 2 * BROAD
            or count % 256 or count > 1024):
        return plain_device(prompt, new_token, w_query, w_key, w_value, decay_rate, norm_gain)
    outer = members // PLANE
    held = HEAD // PLANE
    width = heads * HEAD
    total_rows = count + TOKEN_ROWS
    own = prompt.reshape(count, part)
    swap = [(0, 1), (1, 0)]
    other = lax.ppermute(own, "tp", swap)
    token_other = lax.ppermute(new_token, "tp", swap)
    dma = pltpu.SemaphoreType.DMA

    def call(kernel, name, arguments, specs, outs, out_specs, scratch, flops):
        return pl.pallas_call(kernel, in_specs=specs, out_specs=out_specs, out_shape=outs, scratch_shapes=scratch,
                              compiler_params=params(), cost_estimate=cost(flops), name=name)(*arguments)

    near_cos, near_sin, start_cos, start_sin = angle_tables(count, members)
    near_cos, near_sin, starts = jnp.asarray(near_cos), jnp.asarray(near_sin), jnp.asarray(np.stack([start_cos, start_sin]))
    rows, partial, key_rest, value_rest, cosine, sine, rates = call(
        own_kernel, "own",
        (far(own), far(new_token), far(w_key), far(w_value), far(decay_rate), far(near_cos), far(near_sin), far(starts)),
        [hbm()] * 8,
        [pltpu.VMEM((total_rows, part), bf16), pltpu.VMEM((2 * heads, total_rows, HEAD), f32), pltpu.VMEM((part, width), bf16),
         pltpu.VMEM((part, width), bf16), pltpu.VMEM((total_rows, HEAD), f32), pltpu.VMEM((total_rows, HEAD), f32),
         pltpu.VMEM((heads, HEAD), f32)],
        [vmem()] * 7,
        [pltpu.VMEM((2, part, width), bf16), pltpu.VMEM((1, part), bf16), pltpu.VMEM((2, count, HEAD), f32),
         pltpu.VMEM(starts.shape, f32), pltpu.SMEM((heads,), f32), dma((8 + 2 * width // BROAD,))],
        4 * total_rows * part * width)

    other_rows, turned, values, token_key, token_value, *pieces = call(
        lambda *refs: key_value_kernel(outer, *refs), "key_value",
        (other, token_other, partial, key_rest, value_rest, cosine, sine, rates),
        [vmem()] * 8,
        [pltpu.VMEM((total_rows, part), bf16), pltpu.VMEM((heads, count, HEAD), bf16), pltpu.VMEM((heads, count, HEAD), bf16),
         pltpu.VMEM((heads, TOKEN_ROWS, HEAD), bf16), pltpu.VMEM((heads, TOKEN_ROWS, HEAD), bf16)]
        + [pltpu.VMEM((heads, held, HEAD), bf16)] * PLANE,
        [vmem()] * (5 + PLANE),
        [pltpu.VMEM((heads, count, HEAD), bf16), pltpu.VMEM((heads, PLANE, held, HEAD), f32)],
        4 * total_rows * part * width)

    def plane_swap(items):
        return [items[0]] + [
            lax.ppermute(items[r], "sp", [(s, s ^ r) for s in range(members)]) for r in range(1, PLANE)
        ]

    gathered = plane_swap(pieces)

    late_weights, _ = lax.optimization_barrier((w_query.reshape(2, part, width), turned))
    query_weights = pltpu.with_memory_space_constraint(late_weights, pltpu.VMEM)

    def query(chunk, name, after):
        span = BROAD // HEAD
        return call(
            lambda *refs: query_kernel(outer, chunk, *refs), name,
            (rows, other_rows, query_weights, cosine, sine, after),
            [vmem()] * 5 + [anywhere()],
            [pltpu.VMEM((span, count, HEAD), bf16), pltpu.VMEM((span, TOKEN_ROWS, HEAD), bf16), pltpu.VMEM((span, held, HEAD), f32)],
            [vmem()] * 3,
            [pltpu.VMEM((span, PLANE, held, HEAD), f32)],
            4 * total_rows * part * BROAD)

    scaled_low, token_scaled_low, token_rows_low = query(0, "query_low", rates)

    total, before = call(
        lambda *refs: plane_kernel(count, *refs), "plane",
        (token_scaled_low, rates, *gathered),
        [anywhere()] + [vmem()] * (1 + PLANE),
        [pltpu.VMEM((heads, held, HEAD), bf16), pltpu.VMEM((PLANE, heads, held, HEAD), f32)],
        [vmem()] * 2,
        [pltpu.VMEM((PLANE, heads, held, HEAD), f32)],
        1 << 20)

    totals = [total] + [
        lax.ppermute(total, "sp", [(s, s ^ (PLANE * r)) for s in range(members)]) for r in range(1, outer)
    ]

    scaled_high, token_scaled_high, token_rows_high = query(1, "query_high", total)

    def inside(start, units, name, after):
        return call(
            lambda *refs: inner_kernel(start, *refs), name,
            (rates, scaled_low, scaled_high, turned, values, after),
            [vmem()] * 5 + [anywhere()], [pltpu.VMEM((units, count, HEAD), f32)] * 2, [vmem()] * 2, [],
            4 * count * count * units * HEAD)

    inner_low, fade_low = inside(0, LOW, "inner_low", total)

    *results, final = call(
        lambda *refs: line_kernel(count, outer, *refs), "line",
        (inner_low, rates, *totals, before, token_rows_low, token_rows_high),
        [anywhere()] + [vmem()] * (outer + 4),
        [pltpu.VMEM((heads * held + 2 * heads, HEAD), bf16)] * PLANE + [pltpu.VMEM((heads, held // outer, HEAD), bf16)],
        [vmem()] * (PLANE + 1),
        [pltpu.VMEM((outer, heads, held, HEAD), f32), pltpu.VMEM((heads, outer, held, HEAD), f32),
         pltpu.VMEM((heads, outer, held // outer, HEAD), f32), pltpu.VMEM((2 * heads, HEAD), f32)],
        1 << 20)

    arrived = plane_swap(results)
    inner_high, fade_high = inside(LOW, heads - LOW, "inner_high", results[0])

    mixed, new_read, cache = call(
        lambda *refs: output_kernel(outer, *refs), "output",
        (rates, scaled_low, scaled_high, inner_low, inner_high, fade_low, fade_high, token_scaled_low, token_scaled_high,
         token_key, token_value, final, norm_gain.reshape(1, width), *arrived),
        [vmem()] * (13 + PLANE),
        [shape((count, width), bf16), shape((1, width), bf16), shape((heads, held // outer, HEAD), bf16)],
        [hbm()] * 3,
        [pltpu.VMEM((PLANE, heads * held, HEAD), f32), pltpu.VMEM((PLANE, 2 * heads, HEAD), f32), pltpu.VMEM((1, width), bf16),
         pltpu.VMEM((heads // 2, count, WIDE), bf16), dma((2 + heads // 2,))],
        1 << 20)

    return (mixed.reshape(1, count, width), cache.reshape(1, heads, held // outer, HEAD), new_read)


def shape(dims, dtype):
    return jax.ShapeDtypeStruct(dims, dtype)


def solution(mesh):
    in_specs = (
        P(None, "sp", "tp"),
        P(None, "tp"),
        P(None, "tp"),
        P(None, "tp"),
        P(None, "tp"),
        P("tp"),
        P("tp"),
    )
    out_specs = (P(None, "sp", "tp"), P(None, "tp", "sp", None), P(None, "tp"))
    return jax.shard_map(
        per_device, mesh=mesh, in_specs=in_specs, out_specs=out_specs, check_vma=False
    )
```

```python
import jax
import numpy as np
import jax.numpy as jnp
from jax import lax
from jax.experimental import pallas as pl
from jax.experimental.pallas import tpu as pltpu
from jax.sharding import PartitionSpec as P

HEAD = 128


rope_base = 10000.0
norm_floor = 1e-05


def rotate(tensor, positions):
    head_width = tensor.shape[-1]
    inverse = rope_base ** (-jnp.arange(0, head_width, 2, dtype=jnp.float32) / head_width)
    angles = positions.astype(jnp.float32)[:, None] * inverse[None, :]
    cosine = jnp.cos(angles)[:, None, :]
    sine_part = jnp.sin(angles)[:, None, :]
    first_half = tensor[..., : head_width // 2]
    second_half = tensor[..., head_width // 2 :]
    return jnp.concatenate(
        [
            first_half * cosine - second_half * sine_part,
            first_half * sine_part + second_half * cosine,
        ],
        axis=-1,
    )


def head_norm(output, gain):
    center = jnp.mean(output, axis=-1, keepdims=True)
    spread = jnp.mean(jnp.square(output - center), axis=-1, keepdims=True)
    return (output - center) * lax.rsqrt(spread + norm_floor) * gain


def decay_tables(log_gamma, block_size):
    offsets = jnp.arange(block_size, dtype=jnp.float32)
    gap_table = offsets[:, None] - offsets[None, :]
    within = jnp.where(
        gap_table[None] >= 0,
        jnp.exp(jnp.maximum(gap_table, 0.0)[None] * log_gamma[:, None, None]),
        0.0,
    )
    query_decay = jnp.exp((offsets[:, None] + 1.0) * log_gamma[None, :])
    key_decay = jnp.exp((block_size - 1.0 - offsets[:, None]) * log_gamma[None, :])
    return (within, query_decay, key_decay)


def plain_device(prompt, new_token, w_query, w_key, w_value, decay_rate, norm_gain):
    sequences, block_size, feature_part = prompt.shape
    head_count = w_query.shape[1] // HEAD
    members = lax.axis_size("sp")
    device_rank = lax.axis_index("sp")
    prompt_rows = sequences * block_size
    token_rows = jnp.concatenate([prompt.reshape(prompt_rows, feature_part), new_token], axis=0)
    weight_list = (w_query, w_key, w_value)
    shard_piece = lax.all_gather(token_rows, "tp", axis=1, tiled=True)
    projected = tuple(
        (jnp.dot(shard_piece, weight, preferred_element_type=jnp.float32) for weight in weight_list)
    )
    full_shape = (sequences, block_size, head_count, HEAD)
    queries, key_rows, values = [
        tensor[:prompt_rows].astype(jnp.bfloat16).reshape(full_shape) for tensor in projected
    ]
    token_query, token_key, token_value = [
        tensor[prompt_rows:].astype(jnp.bfloat16).reshape(sequences, 1, head_count, HEAD)
        for tensor in projected
    ]
    positions = device_rank * block_size + jnp.arange(block_size, dtype=jnp.int32)
    scaled = (rotate(queries.astype(jnp.float32), positions) * HEAD ** (-0.5)).astype(jnp.bfloat16)
    turned = rotate(key_rows.astype(jnp.float32), positions).astype(jnp.bfloat16)
    log_gamma = -decay_rate
    within, query_decay, key_decay = decay_tables(log_gamma, block_size)
    weighted = (turned.astype(jnp.float32) * key_decay[None, :, :, None]).astype(jnp.bfloat16)
    local_state = jnp.einsum(
        "smhd,smhe->shde", weighted, values, preferred_element_type=jnp.float32
    )
    pieces = lax.all_to_all(local_state[None], "sp", split_axis=3, concat_axis=0, tiled=True)
    source_index = jnp.arange(members, dtype=jnp.float32)
    gap_table = source_index[:, None] - 1.0 - source_index[None, :]
    weights = jnp.where(
        gap_table[None] >= 0,
        jnp.exp(jnp.maximum(gap_table, 0.0)[None] * block_size * log_gamma[:, None, None]),
        0.0,
    )
    prefix = jnp.einsum("hji,ishre->jshre", weights, pieces, precision=lax.Precision.HIGHEST)
    tail_all = jnp.exp((members - 1.0 - source_index)[None, :] * block_size * log_gamma[:, None])
    final_rows = jnp.einsum("hi,ishre->shre", tail_all, pieces, precision=lax.Precision.HIGHEST)
    incoming = lax.all_to_all(
        prefix.astype(jnp.bfloat16), "sp", split_axis=0, concat_axis=3, tiled=True
    ).astype(prefix.dtype)[0]
    scores = (
        jnp.einsum("snhd,smhd->shnm", scaled, turned, preferred_element_type=jnp.float32)
        * within[None]
    )
    inner_part = jnp.einsum(
        "shnm,smhe->snhe", scores.astype(jnp.bfloat16), values, preferred_element_type=jnp.float32
    )
    carried = (
        jnp.einsum(
            "snhd,shde->snhe",
            scaled,
            incoming.astype(jnp.bfloat16),
            preferred_element_type=jnp.float32,
        )
        * query_decay[None, :, :, None]
    )
    gain = norm_gain.reshape(head_count, HEAD)
    mixed = (
        head_norm(inner_part + carried, gain)
        .astype(jnp.bfloat16)
        .reshape(sequences, block_size, head_count * HEAD)
    )
    cache = final_rows.astype(jnp.bfloat16)
    token_positions = jnp.full((1,), block_size * members, jnp.int32)
    token_scaled = (
        rotate(token_query.astype(jnp.float32), token_positions) * HEAD ** (-0.5)
    ).astype(jnp.bfloat16)[:, 0]
    token_turned = rotate(token_key.astype(jnp.float32), token_positions).astype(jnp.bfloat16)[:, 0]
    row_count = final_rows.shape[2]
    query_rows = lax.dynamic_slice_in_dim(
        token_scaled, device_rank * row_count, row_count, 2
    ).astype(jnp.float32)
    partial_value = jnp.einsum(
        "shr,shre->she", query_rows, final_rows, precision=lax.Precision.HIGHEST
    )
    read_sum = lax.psum(partial_value, "sp")
    own_score = jnp.sum(
        token_scaled.astype(jnp.float32) * token_turned.astype(jnp.float32), axis=-1, keepdims=True
    )
    read_out = jnp.exp(log_gamma)[None, :, None] * read_sum + own_score * token_value[:, 0].astype(
        jnp.float32
    )
    new_read = head_norm(read_out, gain).astype(jnp.bfloat16).reshape(sequences, head_count * HEAD)
    return (mixed, cache, new_read)


PLANE = 4
TOKEN_ROWS = 16
WIDE = 2 * HEAD
BROAD = 4 * HEAD
LOW = 2
f32 = jnp.float32
bf16 = jnp.bfloat16


def vmem():
    return pl.BlockSpec(memory_space=pltpu.VMEM)


def hbm():
    return pl.BlockSpec(memory_space=pltpu.HBM)


def anywhere():
    return pl.BlockSpec(memory_space=pl.ANY)


def far(array):
    return pltpu.with_memory_space_constraint(array, pltpu.HBM)


def params():
    return pltpu.CompilerParams(vmem_limit_bytes=14 * 1024 * 1024)


def cost(flops):
    return pl.CostEstimate(flops=int(flops), transcendentals=0, bytes_accessed=1 << 20)


def place():
    rank = lax.axis_index("sp")
    return rank % PLANE, rank // PLANE


def angle_tables(count, members):
    lane = np.arange(HEAD)
    inverse = rope_base ** (-2.0 * (lane % (HEAD // 2)) / HEAD)
    near = np.arange(count)[:, None] * inverse
    starts = (np.arange(members + 1) * count)[:, None] * inverse
    return [np.float32(f(angles)) for angles in (near, starts) for f in (np.cos, np.sin)]


def own_kernel(own, token_own, w_key, w_value, rate, near_cos, near_sin, starts,
               rows, partial, key_rest, value_rest, cosine, sine, rates,
               weights, token, angles, bases, scalars, sems):
    count, part = own.shape
    width = w_key.shape[1]
    chunks = width // BROAD
    near = pl.ds(pl.multiple_of(lax.axis_index("tp") * part, part), part)
    rest = pl.ds(pl.multiple_of((1 - lax.axis_index("tp")) * part, part), part)
    copies = []

    def copy(source, target):
        copies.append(pltpu.make_async_copy(source, target, sems.at[len(copies)]))
        copies[-1].start()

    copy(token_own, token)
    copy(own, rows.at[pl.ds(0, count), :])
    for index, matrix in enumerate((w_key, w_value)):
        for chunk in range(chunks):
            columns = pl.ds(chunk * BROAD, BROAD)
            copy(matrix.at[near, columns], weights.at[index, :, columns])
    late = len(copies)
    copy(rate, scalars)
    copy(starts, bases)
    copy(near_cos, angles.at[0])
    copy(near_sin, angles.at[1])
    last_tables = len(copies)
    copy(w_key.at[rest, :], key_rest)
    copy(w_value.at[rest, :], value_rest)
    copies[0].wait()
    copies[1].wait()
    rows[pl.ds(count, TOKEN_ROWS), :] = jnp.broadcast_to(token[...], (TOKEN_ROWS, part))
    for index in range(2):
        for chunk in range(chunks):
            columns = slice(chunk * BROAD, (chunk + 1) * BROAD)
            if index == 0:
                copies[2 + chunk].wait()
            elif chunk == 0:
                for item in copies[2 + chunks:late]:
                    item.wait()
            if index == 1 and chunk == 0:
                for item in copies[late:last_tables]:
                    item.wait()
                rank = lax.axis_index("sp")
                last = starts.shape[1] - 1
                sign = jnp.where(lax.broadcasted_iota(jnp.int32, (1, HEAD), 1) < HEAD // 2, -1.0, 1.0)
                base_cos, base_sin = bases[0, pl.ds(rank, 1), :], bases[1, pl.ds(rank, 1), :]
                cosine[pl.ds(0, count), :] = angles[0] * base_cos - angles[1] * base_sin
                sine[pl.ds(0, count), :] = (angles[1] * base_cos + angles[0] * base_sin) * sign
                tail = (TOKEN_ROWS, HEAD)
                cosine[pl.ds(count, TOKEN_ROWS), :] = jnp.broadcast_to(bases[0, last:, :], tail)
                sine[pl.ds(count, TOKEN_ROWS), :] = jnp.broadcast_to(bases[1, last:, :] * sign, tail)
                for head in range(rates.shape[0]):
                    rates[head:head + 1, :] = jnp.full((1, HEAD), scalars[head], f32)
            share = jnp.dot(rows[...], weights[index, :, columns], preferred_element_type=f32)
            for lane in range(BROAD // HEAD):
                partial[(index * width + chunk * BROAD) // HEAD + lane] = share[:, lane * HEAD:(lane + 1) * HEAD]
    for item in copies[last_tables:]:
        item.wait()


def turn(rows, cosine, sine):
    return rows * cosine + pltpu.roll(rows, HEAD // 2, axis=1) * sine


def into_parts(matrix, parts, outer):
    rest = HEAD // (outer * PLANE)
    split = matrix.reshape(outer, PLANE, rest, HEAD)
    for member in range(PLANE):
        parts[member] = split[:, member].reshape(outer * rest, HEAD)


def key_value_kernel(outer, other, token_other, partial, key_rest, value_rest, cosine, sine, rates,
                     rows, turned, values, token_key, token_value, *tail):
    pieces, (weighted, parts) = tail[:PLANE], tail[PLANE:]
    member, _ = place()
    count, part = other.shape
    width = key_rest.shape[1]
    rows[pl.ds(0, count), :] = other[...]
    rows[pl.ds(count, TOKEN_ROWS), :] = jnp.broadcast_to(token_other[...], (TOKEN_ROWS, part))
    offsets = lax.broadcasted_iota(jnp.int32, (count, HEAD), 0).astype(f32)
    lanes = BROAD // HEAD
    for chunk in range(width // BROAD):
        broad = slice(chunk * BROAD, (chunk + 1) * BROAD)
        key_rows = jnp.dot(rows[...], key_rest[:, broad], preferred_element_type=f32)
        for lane in range(lanes):
            head = chunk * lanes + lane
            inside = slice(lane * HEAD, (lane + 1) * HEAD)
            columns = slice(head * HEAD, (head + 1) * HEAD)
            head_rows = (partial[head] + key_rows[:, inside]).astype(bf16).astype(f32)
            result = turn(head_rows, cosine[...], sine[...]).astype(bf16)
            turned[head] = result[:count]
            token_key[head] = result[count:]
            decay = jnp.exp((offsets - (count - 1.0)) * rates[head:head + 1, :])
            weighted[head] = (result[:count].astype(f32) * decay).astype(bf16)
    for chunk in range(width // BROAD):
        broad = slice(chunk * BROAD, (chunk + 1) * BROAD)
        value_rows = jnp.dot(rows[...], value_rest[:, broad], preferred_element_type=f32)
        for lane in range(lanes):
            head = chunk * lanes + lane
            inside = slice(lane * HEAD, (lane + 1) * HEAD)
            columns = slice(head * HEAD, (head + 1) * HEAD)
            head_rows = (partial[width // HEAD + head] + value_rows[:, inside]).astype(bf16)
            values[head] = head_rows[:count]
            token_value[head] = head_rows[count:]
            local = lax.dot_general(weighted[head], head_rows[:count], (((0,), (0,)), ((), ())),
                                    preferred_element_type=f32)
            into_parts(local, parts.at[head], outer)
            for r in range(PLANE):
                pieces[r][head] = parts[head, member ^ r].astype(bf16)


def query_kernel(outer, chunk, own_rows, other_rows, query_weights, cosine, sine, _, scaled, token_scaled, token_rows, parts):
    member, _ = place()
    heads, count, _ = scaled.shape
    side = lax.axis_index("tp")
    broad = slice(chunk * BROAD, (chunk + 1) * BROAD)
    queries = jnp.dot(own_rows[...], query_weights[side, :, broad], preferred_element_type=f32) + jnp.dot(
        other_rows[...], query_weights[1 - side, :, broad], preferred_element_type=f32)
    queries = queries.astype(bf16).astype(f32)
    for head in range(heads):
        inside = slice(head * HEAD, (head + 1) * HEAD)
        result = (turn(queries[:, inside], cosine[...], sine[...]) * HEAD ** (-0.5)).astype(bf16)
        scaled[head] = result[:count]
        token_scaled[head] = result[count:]
        token = jnp.broadcast_to(result[count:].astype(f32)[:1], (HEAD, HEAD))
        into_parts(token.T, parts.at[head], outer)
        token_rows[head] = parts[head, member]


def chosen(low, high, head):
    return (low, head) if head < low.shape[0] else (high, head - low.shape[0])


def inner_kernel(start, rates, scaled_low, scaled_high, turned, values, _, inner, fade):
    heads, count, _ = inner.shape
    half = count // 2
    lanes = lax.broadcasted_iota(jnp.int32, (1, count), 1).astype(f32)
    offsets = lax.broadcasted_iota(jnp.int32, (count, HEAD), 0).astype(f32)
    keep = lax.broadcasted_iota(jnp.int32, (half, half), 0) >= lax.broadcasted_iota(jnp.int32, (half, half), 1)
    center = centering(HEAD)
    for index in range(heads):
        head = start + index
        scaled, at = chosen(scaled_low, scaled_high, head)
        growth = jnp.exp(lanes * rates[head:head + 1, :1])
        decay = jnp.exp(-offsets * rates[head:head + 1, :])
        fade[index] = decay * jnp.exp(-rates[head:head + 1, :])

        def products(n, m):
            raw = lax.dot_general(scaled[at, n * half:(n + 1) * half], turned[head, m * half:(m + 1) * half],
                                  (((1,), (1,)), ((), ())), preferred_element_type=f32)
            raw = raw * growth[:, m * half:(m + 1) * half]
            return (jnp.where(keep, raw, 0.0) if n == m else raw).astype(bf16)

        centered = jnp.dot(values[head], center, preferred_element_type=f32).astype(bf16)
        low, high = centered[:half], centered[half:]
        inner[index, :half] = jnp.dot(products(0, 0), low, preferred_element_type=f32) * decay[:half]
        inner[index, half:] = (jnp.dot(products(1, 0), low, preferred_element_type=f32) + jnp.dot(
            products(1, 1), high, preferred_element_type=f32)) * decay[half:]


def plane_kernel(count, _, rates, *refs):
    pieces, (total, before, parts) = refs[:PLANE], refs[PLANE:]
    member, _ = place()
    for r in range(PLANE):
        parts[member ^ r] = pieces[r][...].astype(f32)
    for head in range(total.shape[0]):
        factor = jnp.exp(rates[head:head + 1, :] * -count)
        state = jnp.zeros(total.shape[1:], f32)
        for source in range(PLANE):
            before[source, head] = state
            state = state * factor + parts[source, head]
        total[head] = state.astype(bf16)


def line_kernel(count, outer, _, rates, *refs):
    totals = refs[:outer]
    before, token_rows_low, token_rows_high = refs[outer:outer + 3]
    results, cache = refs[outer + 3:outer + 3 + PLANE], refs[outer + 3 + PLANE]
    ordered, running, final, reads = refs[outer + 4 + PLANE:]
    member, line = place()
    heads, width = totals[0].shape[:2]
    for s in range(outer):
        ordered[line ^ s] = totals[s][...].astype(f32)
    for head in range(heads):
        log_factor = rates[head:head + 1, :] * -count
        factor = jnp.exp(log_factor * PLANE)
        state = jnp.zeros((width, HEAD), f32)
        for source in range(outer):
            running[head, source] = state
            state = state * factor + ordered[source, head]
        final[head] = state.reshape(final.shape[1:])
        cache[head] = final[head, line].astype(bf16)
        token_rows, at = chosen(token_rows_low, token_rows_high, head)
        read = jnp.sum(token_rows[at] * state, axis=0, keepdims=True)
        high = read.astype(bf16).astype(f32)
        reads[head:head + 1, :] = high
        reads[heads + head:heads + head + 1, :] = read - high
        arriving = running[head, line]
        for r in range(PLANE):
            scale = jnp.exp(log_factor * (member ^ r).astype(f32))
            results[r][pl.ds(head * width, width), :] = (before[member ^ r, head] + scale * arriving).astype(bf16)
    for r in range(PLANE):
        results[r][pl.ds(heads * width, 2 * heads), :] = reads[...].astype(bf16)


def centering(size):
    rows_of = lax.broadcasted_iota(jnp.int32, (size, size), 0)
    columns_of = lax.broadcasted_iota(jnp.int32, (size, size), 1)
    same = jnp.where(rows_of == columns_of, 1.0, 0.0)
    return (same - jnp.where(rows_of // HEAD == columns_of // HEAD, 1.0 / HEAD, 0.0)).astype(bf16)


def finish(rows, gain):
    center = jnp.mean(rows, axis=-1, keepdims=True)
    rows = rows - center
    spread = jnp.mean(jnp.square(rows), axis=-1, keepdims=True)
    return rows * lax.rsqrt(spread + norm_floor) * gain


def output_kernel(outer, rates, scaled_low, scaled_high, inner_low, inner_high, fade_low, fade_high,
                  token_scaled_low, token_scaled_high, token_key, token_value, final, gain, *refs):
    pieces, (mixed, new_read, cache, parts, reads, read_buffer, buffer, sems) = refs[:PLANE], refs[PLANE:]
    member, _ = place()
    heads, count, _ = token_key.shape[0], scaled_low.shape[1], 0
    held = HEAD // PLANE
    copies = [pltpu.make_async_copy(final, cache, sems.at[0])]
    copies[0].start()
    for r in range(PLANE):
        parts[member ^ r] = pieces[r][pl.ds(0, heads * held), :].astype(f32)
        reads[member ^ r] = pieces[r][pl.ds(heads * held, 2 * heads), :].astype(f32)
    sums = reads[0]
    for source in range(1, PLANE):
        sums = sums + reads[source]
    sums = sums[:heads] + sums[heads:]
    for head in range(heads):
        columns = slice(head * HEAD, (head + 1) * HEAD)
        token_scaled, at = chosen(token_scaled_low, token_scaled_high, head)
        query = token_scaled[at].astype(f32)[:1]
        key = token_key[head].astype(f32)[:1]
        value = token_value[head].astype(f32)[:1]
        own_score = jnp.sum(query * key, axis=-1, keepdims=True)
        read = jnp.exp(-rates[head:head + 1, :]) * sums[head:head + 1] + own_score * value
        read_buffer[:, columns] = finish(read, gain[:, columns]).astype(bf16)
    copies.append(pltpu.make_async_copy(read_buffer, new_read, sems.at[1]))
    copies[1].start()
    rows_of = lax.broadcasted_iota(jnp.int32, (WIDE, WIDE), 0) // HEAD
    columns_of = lax.broadcasted_iota(jnp.int32, (WIDE, WIDE), 1) // HEAD
    average = jnp.where(rows_of == columns_of, 1.0 / HEAD, 0.0).astype(bf16)
    center = centering(HEAD)
    blank = jnp.zeros((HEAD, HEAD), bf16)

    def both(low, high, head):
        sides = [chosen(low, high, head), chosen(low, high, head + 1)]
        return jnp.concatenate([side[at] for side, at in sides], axis=1)

    for pair in range(heads // 2):
        wide = slice(pair * WIDE, (pair + 1) * WIDE)
        states = []
        for head in (2 * pair, 2 * pair + 1):
            split = [parts[source, pl.ds(head * held, held), :].reshape(outer, 1, held // outer, HEAD) for source in range(PLANE)]
            state = jnp.concatenate(split, axis=1).reshape(HEAD, HEAD).astype(bf16)
            states.append(jnp.dot(state, center, preferred_element_type=f32).astype(bf16))
        incoming = jnp.concatenate([jnp.concatenate([states[0], blank], axis=1), jnp.concatenate([blank, states[1]], axis=1)], axis=0)
        carried = jnp.dot(both(scaled_low, scaled_high, 2 * pair), incoming, preferred_element_type=f32)
        rows = both(inner_low, inner_high, 2 * pair) + carried * both(fade_low, fade_high, 2 * pair)
        spread = jnp.dot((rows * rows).astype(bf16), average, preferred_element_type=f32)
        buffer[pair] = (rows * lax.rsqrt(spread + norm_floor) * gain[:, wide]).astype(bf16)
        copies.append(pltpu.make_async_copy(buffer.at[pair], mixed.at[:, pl.ds(pair * WIDE, WIDE)], sems.at[2 + pair]))
        copies[-1].start()
    for copy in copies:
        copy.wait()


def per_device(prompt, new_token, w_query, w_key, w_value, decay_rate, norm_gain):
    members = lax.axis_size("sp")
    heads = w_query.shape[1] // HEAD
    sequences, count, part = prompt.shape
    if (lax.axis_size("tp") != 2 or members % PLANE or HEAD % (8 * members) or sequences != 1 or heads * HEAD != 2 * BROAD
            or count % 256 or count > 1024):
        return plain_device(prompt, new_token, w_query, w_key, w_value, decay_rate, norm_gain)
    outer = members // PLANE
    held = HEAD // PLANE
    width = heads * HEAD
    total_rows = count + TOKEN_ROWS
    own = prompt.reshape(count, part)
    swap = [(0, 1), (1, 0)]
    other = lax.ppermute(own, "tp", swap)
    token_other = lax.ppermute(new_token, "tp", swap)
    dma = pltpu.SemaphoreType.DMA

    def call(kernel, name, arguments, specs, outs, out_specs, scratch, flops):
        return pl.pallas_call(kernel, in_specs=specs, out_specs=out_specs, out_shape=outs, scratch_shapes=scratch,
                              compiler_params=params(), cost_estimate=cost(flops), name=name)(*arguments)

    near_cos, near_sin, start_cos, start_sin = angle_tables(count, members)
    near_cos, near_sin, starts = jnp.asarray(near_cos), jnp.asarray(near_sin), jnp.asarray(np.stack([start_cos, start_sin]))
    rows, partial, key_rest, value_rest, cosine, sine, rates = call(
        own_kernel, "own",
        (far(own), far(new_token), far(w_key), far(w_value), far(decay_rate), far(near_cos), far(near_sin), far(starts)),
        [hbm()] * 8,
        [pltpu.VMEM((total_rows, part), bf16), pltpu.VMEM((2 * heads, total_rows, HEAD), f32), pltpu.VMEM((part, width), bf16),
         pltpu.VMEM((part, width), bf16), pltpu.VMEM((total_rows, HEAD), f32), pltpu.VMEM((total_rows, HEAD), f32),
         pltpu.VMEM((heads, HEAD), f32)],
        [vmem()] * 7,
        [pltpu.VMEM((2, part, width), bf16), pltpu.VMEM((1, part), bf16), pltpu.VMEM((2, count, HEAD), f32),
         pltpu.VMEM(starts.shape, f32), pltpu.SMEM((heads,), f32), dma((8 + 2 * width // BROAD,))],
        4 * total_rows * part * width)

    other_rows, turned, values, token_key, token_value, *pieces = call(
        lambda *refs: key_value_kernel(outer, *refs), "key_value",
        (other, token_other, partial, key_rest, value_rest, cosine, sine, rates),
        [vmem()] * 8,
        [pltpu.VMEM((total_rows, part), bf16), pltpu.VMEM((heads, count, HEAD), bf16), pltpu.VMEM((heads, count, HEAD), bf16),
         pltpu.VMEM((heads, TOKEN_ROWS, HEAD), bf16), pltpu.VMEM((heads, TOKEN_ROWS, HEAD), bf16)]
        + [pltpu.VMEM((heads, held, HEAD), bf16)] * PLANE,
        [vmem()] * (5 + PLANE),
        [pltpu.VMEM((heads, count, HEAD), bf16), pltpu.VMEM((heads, PLANE, held, HEAD), f32)],
        4 * total_rows * part * width)

    def plane_swap(items):
        return [items[0]] + [
            lax.ppermute(items[r], "sp", [(s, s ^ r) for s in range(members)]) for r in range(1, PLANE)
        ]

    gathered = plane_swap(pieces)

    late_weights, _ = lax.optimization_barrier((w_query.reshape(2, part, width), turned))
    query_weights = pltpu.with_memory_space_constraint(late_weights, pltpu.VMEM)

    def query(chunk, name, after):
        span = BROAD // HEAD
        return call(
            lambda *refs: query_kernel(outer, chunk, *refs), name,
            (rows, other_rows, query_weights, cosine, sine, after),
            [vmem()] * 5 + [anywhere()],
            [pltpu.VMEM((span, count, HEAD), bf16), pltpu.VMEM((span, TOKEN_ROWS, HEAD), bf16), pltpu.VMEM((span, held, HEAD), f32)],
            [vmem()] * 3,
            [pltpu.VMEM((span, PLANE, held, HEAD), f32)],
            4 * total_rows * part * BROAD)

    scaled_low, token_scaled_low, token_rows_low = query(0, "query_low", rates)

    total, before = call(
        lambda *refs: plane_kernel(count, *refs), "plane",
        (token_scaled_low, rates, *gathered),
        [anywhere()] + [vmem()] * (1 + PLANE),
        [pltpu.VMEM((heads, held, HEAD), bf16), pltpu.VMEM((PLANE, heads, held, HEAD), f32)],
        [vmem()] * 2,
        [pltpu.VMEM((PLANE, heads, held, HEAD), f32)],
        1 << 20)

    totals = [total] + [
        lax.ppermute(total, "sp", [(s, s ^ (PLANE * r)) for s in range(members)]) for r in range(1, outer)
    ]

    scaled_high, token_scaled_high, token_rows_high = query(1, "query_high", total)

    def inside(start, units, name, after):
        return call(
            lambda *refs: inner_kernel(start, *refs), name,
            (rates, scaled_low, scaled_high, turned, values, after),
            [vmem()] * 5 + [anywhere()], [pltpu.VMEM((units, count, HEAD), f32)] * 2, [vmem()] * 2, [],
            4 * count * count * units * HEAD)

    inner_low, fade_low = inside(0, LOW, "inner_low", total)

    *results, final = call(
        lambda *refs: line_kernel(count, outer, *refs), "line",
        (inner_low, rates, *totals, before, token_rows_low, token_rows_high),
        [anywhere()] + [vmem()] * (outer + 4),
        [pltpu.VMEM((heads * held + 2 * heads, HEAD), bf16)] * PLANE + [pltpu.VMEM((heads, held // outer, HEAD), bf16)],
        [vmem()] * (PLANE + 1),
        [pltpu.VMEM((outer, heads, held, HEAD), f32), pltpu.VMEM((heads, outer, held, HEAD), f32),
         pltpu.VMEM((heads, outer, held // outer, HEAD), f32), pltpu.VMEM((2 * heads, HEAD), f32)],
        1 << 20)

    arrived = plane_swap(results)
    inner_high, fade_high = inside(LOW, heads - LOW, "inner_high", results[0])

    mixed, new_read, cache = call(
        lambda *refs: output_kernel(outer, *refs), "output",
        (rates, scaled_low, scaled_high, inner_low, inner_high, fade_low, fade_high, token_scaled_low, token_scaled_high,
         token_key, token_value, final, norm_gain.reshape(1, width), *arrived),
        [vmem()] * (13 + PLANE),
        [shape((count, width), bf16), shape((1, width), bf16), shape((heads, held // outer, HEAD), bf16)],
        [hbm()] * 3,
        [pltpu.VMEM((PLANE, heads * held, HEAD), f32), pltpu.VMEM((PLANE, 2 * heads, HEAD), f32), pltpu.VMEM((1, width), bf16),
         pltpu.VMEM((heads // 2, count, WIDE), bf16), dma((2 + heads // 2,))],
        1 << 20)

    return (mixed.reshape(1, count, width), cache.reshape(1, heads, held // outer, HEAD), new_read)


def shape(dims, dtype):
    return jax.ShapeDtypeStruct(dims, dtype)


def solution(mesh):
    in_specs = (
        P(None, "sp", "tp"),
        P(None, "tp"),
        P(None, "tp"),
        P(None, "tp"),
        P(None, "tp"),
        P("tp"),
        P("tp"),
    )
    out_specs = (P(None, "sp", "tp"), P(None, "tp", "sp", None), P(None, "tp"))
    return jax.shard_map(
        per_device, mesh=mesh, in_specs=in_specs, out_specs=out_specs, check_vma=False
    )
```
